32 devices in a mesh: ep: 8 (over z, x), tp: 4 (over y, core).
Axes of the slice: x: 2, y: 2, z: 4, core: 2. Of those that a mesh axis runs over, the one named last changes fastest.
Arguments:
- tokens: bfloat16 [4096, 4096], P('ep', 'tp'), may hold values from -100 to 100, as said below
- routes: int32 [4096, 2], P('ep'), may hold values from 0 to 15, all different within a row; in each aligned block of 512 rows (0 to 511, 512 to 1023, ...) at most 128 rows name the same one
- route_weights: float32 [4096, 2], P('ep'), may hold values from 0.1 to 1
- norm_gain: float32 [4096], P('tp'), may hold values from 0.1 to 1.9
- gate_weight: bfloat16 [16, 4096, 512], P('ep', 'tp'), may hold values from -0.09375 to 0.09375
- up_weight: bfloat16 [16, 4096, 512], P('ep', 'tp'), may hold values from -0.09375 to 0.09375
- down_weight: bfloat16 [16, 512, 4096], P('ep', None, 'tp'), may hold values from -0.25 to 0.25
- final_gain: float32 [4096], P('tp'), may hold values from 0.1 to 1.9
Outputs:
- mixed: bfloat16 [4096, 4096], P('ep', 'tp')
The draws below stay inside these ranges and needn't reach their ends.
Inputs may be any that keep to these rules, and one draw needn't show every extreme that they name: `tokens`: real-valued activations whose features differ in scale. `routes`: each row names 2 different experts; among the 512 rows of one aligned block no expert is named more than 128 times, a bound that some block reaches.
All inputs are finite; a program needn't handle non-finite values.
Results may differ from the reference program's by a relative error of at most 0.018.
Values may be sent and summed in bfloat16 or wider, within the bound.
A program may use at most 64 MiB of HBM per device.

```python
import math
import jax
import jax.numpy as jnp
import numpy as np
from jax import lax

D = 4096
FF = 512
TOP = 2
TOK_DEV = 512
EXPERTS = 16
CAP = 128
TOKENS = 4096
N_EP = 8
N_TP = 4


def draw_tokens(key, part):
    keys = jax.random.split(jax.random.fold_in(key, 11), 2)
    column = jnp.exp(jnp.log(6.0) * jnp.arange(D, dtype=jnp.float32) / (D - 1))
    row_scale = jnp.exp(jax.random.uniform(keys[1], (TOKENS, 1), jnp.float32, 0.0, jnp.log(10.0)))
    base = jax.random.normal(keys[0], (TOKENS, D), jnp.float32)
    base = jnp.clip(base, -5.0, 5.0)
    return (base * column * row_scale / 3.0).astype(jnp.bfloat16)


def shard_levels(own_key, dims, shards, smallest, high):
    loudness = 1.0
    for dim, blocks in shards:
        draws = jax.random.uniform(jax.random.fold_in(jax.random.fold_in(own_key, 6), dim), (blocks,), jnp.float32, smallest / len(shards), high / len(shards))
        loudness = loudness * jnp.repeat(jnp.exp(draws), dims[dim] // blocks).reshape((-1,) + (1,) * (len(dims) - 1 - dim))
    return loudness


def assign_block(key, own, number, rows, amount, top, limit, skew):
    order = jax.random.permutation(key, amount)
    crowded, ordinary = shares(amount, rows * top, limit, skew, True), shares(amount, rows * top, limit, skew, False)
    places = jnp.arange(amount)

    def named(tallies, offset_by):
        used = int((tallies > 0).sum())
        fixed = max(1, used // 4)
        shifted = fixed + (places - fixed + offset_by * (used - fixed)) % max(1, amount - fixed)
        return jnp.zeros((amount,), jnp.int32).at[order[jnp.where(places < fixed, places, shifted)]].set(jnp.asarray(tallies, jnp.int32))

    tallies = jnp.where(number % 4 == 0, named(crowded, number // 4), named(ordinary, number - number // 4 - 1))
    mixed = jax.random.permutation(jax.random.fold_in(own, 3), amount)
    source_of, sink = mixed[0:amount // 2 * 2:2], mixed[1:amount // 2 * 2:2]
    room = jnp.minimum(tallies[source_of] - 1, limit - tallies[sink]) // 2
    room = jnp.where((source_of == order[0]) | (sink == order[0]) | (tallies[sink] == 0), 0, jnp.maximum(room, 0))
    shifted = jax.random.randint(jax.random.fold_in(own, 4), (amount // 2,), 0, 1 << 20) % (room + 1)
    tallies = tallies.at[source_of].add(-shifted).at[sink].add(shifted)
    labels = jnp.searchsorted(jnp.cumsum(tallies), jnp.arange(rows * top), side="right").astype(jnp.int32)
    listing = labels.reshape(top, rows).T
    listing = listing[jax.random.permutation(jax.random.fold_in(own, 1), rows)]
    offset_by = jax.random.randint(jax.random.fold_in(own, 2), (rows, 1), 0, top)
    return jnp.take_along_axis(listing, (jnp.arange(top)[None, :] + offset_by) % top, axis=1)


def shares(amount, total, reach, lean, full):
    loads = [(1 << 20) // math.isqrt(grade ** lean) + 1 for grade in range(1, amount + 1)]
    largest = reach if full else min(reach, max(-(-total // amount), total * loads[0] // sum(loads)))
    least = 1 if total - largest >= amount - 1 else 0
    given, surplus = [largest] + [least] * (amount - 1), total - largest - least * (amount - 1)
    while surplus > 0:
        candidates = [i for i in range(1, amount) if given[i] < largest] or [i for i in range(1, amount) if given[i] < reach]
        pool, left = sum([loads[i] for i in candidates]), surplus
        for i in candidates:
            addition = min(reach - given[i], max(1, left * loads[i] // pool), surplus)
            given[i] = given[i] + addition
            surplus = surplus - addition
    return np.array(given)


def noise(key, shape, scale, bound, pieces=(), kind=jnp.bfloat16):
    result = scale * jax.random.normal(key, shape, jnp.float32)
    if pieces:
        result = result * shard_levels(key, shape, pieces, -0.22, 0.18)
    return jnp.clip(result, -bound, bound).astype(kind)


def setup_inputs(seed: int = 0) -> dict:
    arg_keys = jax.random.split(jax.random.key(seed), 9)
    tokens = draw_tokens(jax.random.fold_in(arg_keys[8], 71), 0)
    routes_keys = jax.random.split(jax.random.fold_in(arg_keys[1], 1), TOKENS // TOK_DEV)
    routes_turns = jax.random.permutation(jax.random.fold_in(arg_keys[1], 3), TOKENS // TOK_DEV)
    routes = jax.vmap(lambda own, number: assign_block(jax.random.fold_in(arg_keys[1], 2), own, number, TOK_DEV, EXPERTS, TOP, CAP, 2))(routes_keys, routes_turns).reshape((TOKENS, TOP))
    route_weights = jnp.clip(0.1 + 0.9 * jax.random.uniform(arg_keys[2], (TOKENS, TOP), jnp.float32) ** shard_levels(arg_keys[2], (TOKENS, TOP), ((0, 8),), -0.2, 0.2), 0.1, 1.0)
    norm_gain = jnp.clip(1.0 + 0.18 * jax.random.normal(arg_keys[3], (D,), jnp.float32), 0.1, 1.9)
    gate_weight = noise(arg_keys[4], (EXPERTS, D, FF), D ** -0.5, 0.09375, ((0, 8), (1, 4)))
    up_weight = noise(arg_keys[5], (EXPERTS, D, FF), D ** -0.5, 0.09375, ((0, 8), (1, 4)))
    down_weight = noise(arg_keys[6], (EXPERTS, FF, D), FF ** -0.5, 0.25, ((0, 8), (2, 4)))
    final_gain = jnp.clip(1.0 + 0.18 * jax.random.normal(arg_keys[7], (D,), jnp.float32), 0.1, 1.9)
    return {"tokens": tokens, "routes": routes, "route_weights": route_weights, "norm_gain": norm_gain, "gate_weight": gate_weight, "up_weight": up_weight, "down_weight": down_weight, "final_gain": final_gain}


EPSILON = 1e-06

def slots_of(chosen):
    experts = jnp.arange(EXPERTS, dtype=jnp.int32)
    onehot = (chosen[:, None] == experts[None, :]).astype(jnp.int32)
    before = jnp.cumsum(onehot, axis=0) - onehot
    return lax.optimization_barrier(jnp.sum(before * onehot, axis=1)).astype(jnp.int32)

def reference(tokens, routes, route_weights, norm_gain, gate_weight, up_weight, down_weight, final_gain):
    values = tokens.astype(jnp.float32)
    scale = lax.rsqrt(lax.optimization_barrier(jnp.mean(values * values, axis=-1, keepdims=True)) + EPSILON)
    normed = (values * scale * norm_gain).astype(jnp.bfloat16)
    count = tokens.shape[0]
    blocks = routes.reshape(N_EP, TOK_DEV * TOP)
    slots = jax.vmap(slots_of)(blocks)
    source = jnp.broadcast_to(jnp.arange(N_EP, dtype=jnp.int32)[:, None], blocks.shape)
    owner = source * TOK_DEV + jnp.arange(TOK_DEV * TOP, dtype=jnp.int32)[None, :] // TOP
    table = jnp.full((EXPERTS, N_EP, CAP), count, jnp.int32).at[blocks, source, slots].set(owner)
    padded = jnp.concatenate([normed, jnp.zeros((1, D), jnp.bfloat16)], axis=0)
    block_width = D // N_TP

    def one_expert(operands):
        index, w_gate, w_up, w_down = operands
        rows = padded[index.reshape(-1)]
        gate = jnp.zeros((rows.shape[0], FF), jnp.float32)
        upper = jnp.zeros((rows.shape[0], FF), jnp.float32)
        for quarter in range(N_TP):
            lower_col = quarter * block_width
            part_rows = rows[:, lower_col:lower_col + block_width]
            gate = gate + jnp.dot(part_rows, w_gate[lower_col:lower_col + block_width], preferred_element_type=jnp.float32).astype(jnp.bfloat16).astype(jnp.float32)
            upper = upper + jnp.dot(part_rows, w_up[lower_col:lower_col + block_width], preferred_element_type=jnp.float32).astype(jnp.bfloat16).astype(jnp.float32)
        hidden = (jax.nn.silu(gate) * upper).astype(jnp.bfloat16)
        return jnp.dot(hidden, w_down, preferred_element_type=jnp.float32).astype(jnp.bfloat16)
    outputs = lax.map(one_expert, (table, gate_weight, up_weight, down_weight))
    returned = outputs.reshape(EXPERTS * N_EP * CAP, D)
    position = (blocks * (N_EP * CAP) + source * CAP + slots).reshape(count, TOP)
    combined = jnp.zeros((count, D), jnp.float32)
    for which in range(TOP):
        combined = combined + route_weights[:, which:which + 1] * returned[position[:, which]].astype(jnp.float32)
    closing = lax.rsqrt(lax.optimization_barrier(jnp.mean(combined * combined, axis=-1, keepdims=True)) + EPSILON)
    return (combined * closing * final_gain).astype(jnp.bfloat16)
```

```python
import functools

import jax
import jax.numpy as jnp
from jax import lax
from jax.experimental import pallas as pl
from jax.experimental.pallas import tpu as pltpu
from jax.sharding import PartitionSpec as P

EPSILON = 1e-06
BF = jnp.bfloat16
F32 = jnp.float32


def dot(a, b):
    return jnp.dot(a, b, preferred_element_type=F32)


def dot_t(a, b):
    return lax.dot_general(a, b, (((0,), (0,)), ((), ())), preferred_element_type=F32)


def kernel(
    n, nt, local, cap, ring, full,
    x_ref, meta_ref, gain_ref, last_gain_ref, gate_hbm, up_hbm, down_hbm, out_ref,
    gate_v, up_v, down_v, xn, acc, tri, rank_t, wt_t, sq, sq2,
    send_x, recv_x, pk_s, pk_r, far_r, meta_r,
    part, recv_p, hid, out_s, out_r,
    w_sem, xs_sem, xr_sem, ks_sem, kr_sem, fs_sem, fr_sem, ms_sem, mr_sem,
    ps_sem, pr_sem, hs_sem, hr_sem, os_sem, or_sem, qs_sem, qr_sem,
):
    me = lax.axis_index("ep")
    my_tp = lax.axis_index("tp")
    ff = gate_v.shape[2]
    fq = ff // nt
    rows_all = x_ref.shape[0]
    half = n // 2
    chunk = rows_all // 2
    count = local * cap
    split = local // 2

    loads = [
        pltpu.make_async_copy(src, dst, w_sem.at[i])
        for i, (src, dst) in enumerate(((gate_hbm, gate_v), (up_hbm, up_v), (down_hbm, down_v)))
    ]
    for load in loads:
        load.start()

    barrier = pltpu.get_barrier_semaphore()

    @pl.loop(1, n)
    def _(s):
        pl.semaphore_signal(barrier, inc=1, device_id={"ep": lax.rem(me + s, n), "tp": my_tp})

    for o in range(1, nt):
        pl.semaphore_signal(barrier, inc=1, device_id={"ep": me, "tp": lax.rem(my_tp + o, nt)})

    place = jnp.where(me % 2 == 0, me // 2, n - 1 - me // 2)

    def at_place(p):
        p = lax.rem(p + 2 * n, n)
        return jnp.where(p < half, 2 * p, 2 * (n - 1 - p) + 1)

    def shift(s):
        return (1 - 2 * ((s + 1) % 2)) * ((s + 1) // 2)

    def source(s):
        if ring:
            return at_place(place - shift(s))
        return lax.rem(me - s + n, n)

    def sender(s):
        if ring:
            return at_place(place + shift(s))
        return lax.rem(me + s, n)

    def eye():
        shape = (rows_all, rows_all)
        return lax.broadcasted_iota(jnp.int32, shape, 0) == lax.broadcasted_iota(jnp.int32, shape, 1)

    def sq_copy(k, o):
        q = lax.rem(my_tp + o, nt)
        return pltpu.make_async_remote_copy(
            sq.at[k], sq2.at[k, o - 1], qs_sem.at[k, o - 1], qr_sem.at[k, o - 1],
            device_id={"ep": me, "tp": q},
        )

    def start_sum(k, column):
        row = jnp.sum(jnp.where(eye(), column, 0.0), axis=0, keepdims=True)
        sq[k] = jnp.broadcast_to(row, sq.shape[1:])

    def send_sum(k):
        for o in range(1, nt):
            sq_copy(k, o).start()

    def finish_sum(k):
        for o in range(1, nt):
            sq_copy(k, o).wait_recv()
        total = sq[k]
        for o in range(1, nt):
            total = total + sq2[k, o - 1]
        scale = lax.rsqrt(total[0:1] / full + EPSILON)
        return jnp.sum(jnp.where(eye(), scale, 0.0), axis=1, keepdims=True)

    def make_table(slot, meta):
        names = lax.broadcasted_iota(jnp.int32, rank_t.shape[1:], 0).astype(F32)
        first, second = meta[0:1] == names, meta[1:2] == names
        hit = first | second
        before = dot(jnp.where(hit, 1.0, 0.0).astype(BF), tri[...])
        rank_t[slot] = jnp.where(hit, before, -1.0)
        wt_t[slot] = jnp.where(first, meta[2:3], 0.0) + jnp.where(second, meta[3:4], 0.0)

    def onehot(slot, expert, weighted=False):
        rank = rank_t[slot, pl.ds(expert, 1), :]
        hit = lax.broadcasted_iota(jnp.int32, (cap, rows_all), 0).astype(F32) == rank
        return jnp.where(hit, wt_t[slot, pl.ds(expert, 1), :] if weighted else F32(1.0), F32(0.0))

    def pack(slot, experts, block):
        pick = jnp.concatenate([onehot(slot, e) for e in experts], axis=0).astype(BF)
        return dot(pick, block).astype(BF)

    def experts_of(owner):
        return [owner * local + j for j in range(local)]

    def x_copy(s):
        return pltpu.make_async_remote_copy(
            send_x.at[s], recv_x.at[s], xs_sem.at[s], xr_sem.at[s],
            device_id={"ep": sender(s), "tp": my_tp},
        )

    def ahead(i):
        return {"ep": at_place(place + 1 - 2 * i), "tp": my_tp}

    def block_copy(d, i, k):
        piece = pl.ds(k * chunk, chunk)
        src = xn.at[piece] if d == 1 else recv_x.at[2 * d - 4 + i, piece]
        slot = 2 * d - 2 + i
        return pltpu.make_async_remote_copy(
            src, recv_x.at[slot, piece], xs_sem.at[slot, k], xr_sem.at[slot, k], device_id=ahead(i)
        )

    def meta_copy(d, i):
        slot = 2 * d - 2 + i
        return pltpu.make_async_remote_copy(
            meta_ref if d == 1 else meta_r.at[slot - 2], meta_r.at[slot],
            ms_sem.at[slot], mr_sem.at[slot], device_id=ahead(i),
        )

    def pack_copy(i):
        return pltpu.make_async_remote_copy(
            pk_s.at[i], pk_r.at[i], ks_sem.at[i], kr_sem.at[i], device_id=ahead(i)
        )

    def far_copy(i):
        return pltpu.make_async_remote_copy(
            pk_r.at[i, pl.ds(count, split * cap)], far_r.at[i], fs_sem.at[i], fr_sem.at[i],
            device_id=ahead(i),
        )

    def p_copy(s, o):
        q = lax.rem(my_tp + o, nt)
        return pltpu.make_async_remote_copy(
            part.at[s, q], recv_p.at[s, o - 1], ps_sem.at[s, o - 1], pr_sem.at[s, o - 1],
            device_id={"ep": me, "tp": q},
        )

    def h_copy(s, o, back=False):
        mine = lax.rem(my_tp - o + nt, nt) if back else my_tp
        q = lax.rem(my_tp - o + nt, nt) if back else lax.rem(my_tp + o, nt)
        return pltpu.make_async_remote_copy(
            hid.at[s, mine], hid.at[s, mine], hs_sem.at[s, o - 1], hr_sem.at[s, o - 1],
            device_id={"ep": me, "tp": q},
        )

    def o_copy(s):
        return pltpu.make_async_remote_copy(
            out_s.at[s], out_r.at[s], os_sem.at[s], or_sem.at[s],
            device_id={"ep": source(s), "tp": my_tp},
        )

    def stage_a(s, rows_of):
        for j in range(local):
            rows = rows_of(j)
            gate = dot(rows, gate_v[j]).astype(BF)
            upper = dot(rows, up_v[j]).astype(BF)
            for q in range(nt):
                part[s, q, pl.ds(j * cap, cap), pl.ds(0, fq)] = gate[:, q * fq:(q + 1) * fq]
                part[s, q, pl.ds(j * cap, cap), pl.ds(fq, fq)] = upper[:, q * fq:(q + 1) * fq]
        for o in range(1, nt):
            p_copy(s, o).start()

    def stage_b(s):
        for o in range(1, nt):
            p_copy(s, o).wait_recv()
        total = part[s, my_tp].astype(F32)
        for o in range(1, nt):
            total = total + recv_p[s, o - 1].astype(F32)
        gate, upper = total[:, :fq], total[:, fq:]
        hid[s, my_tp] = (gate / (1.0 + jnp.exp(-gate)) * upper).astype(BF)
        for o in range(1, nt):
            h_copy(s, o).start()

    def stage_c(s, own):
        for o in range(1, nt):
            h_copy(s, o, True).wait_recv()
        target = out_r if own else out_s
        for j in range(local):
            hidden = jnp.concatenate([hid[s, q, pl.ds(j * cap, cap), :] for q in range(nt)], axis=1)
            target[s, pl.ds(j * cap, cap), :] = dot(hidden, down_v[j]).astype(BF)
        if not own:
            o_copy(s).start()

    def combine(s):
        weight = jnp.concatenate([onehot(0, e, True) for e in experts_of(sender(s))], axis=0)
        high = weight.astype(BF)
        low = (weight - high.astype(F32)).astype(BF)
        rows = out_r[s]
        return dot_t(high, rows) + dot_t(low, rows)

    values = x_ref[...].astype(F32)
    start_sum(0, jnp.sum(values * values, axis=1, keepdims=True))
    shape = (rows_all, rows_all)
    earlier = lax.broadcasted_iota(jnp.int32, shape, 0) < lax.broadcasted_iota(jnp.int32, shape, 1)
    tri[...] = jnp.where(earlier, 1.0, 0.0).astype(BF)
    pl.semaphore_wait(barrier, n - 1 + nt - 1)
    send_sum(0)
    if ring:
        for i in range(2):
            meta_copy(1, i).start()
    make_table(0, meta_ref[...])
    scale = finish_sum(0)
    xn[...] = (x_ref[...].astype(F32) * scale * gain_ref[...]).astype(BF)

    def own_rows(j):
        return pack(0, [me * local + j], xn[...])

    def stored(ref, slot):
        return lambda j: ref[slot, pl.ds(j * cap, cap), :]

    if ring:
        for k in range(2):
            for i in range(2):
                block_copy(1, i, k).start()
        for load in loads:
            load.wait()
        stage_a(0, own_rows)
        for d in range(1, half + 1):
            if d <= half - 2:
                for k in range(2):
                    for i in range(2):
                        block_copy(d, i, k).wait_recv()
                        if d < half - 2:
                            block_copy(d + 1, i, k).start()
                for i in range(2):
                    slot = 2 * d - 2 + i
                    meta_copy(d, i).wait_recv()
                    if d < half - 2:
                        meta_copy(d + 1, i).start()
                    make_table(1 + slot, meta_r[slot])
                if d == half - 2:
                    for i in range(2):
                        slot = 2 * d - 2 + i
                        step = 1 - 2 * i
                        far = experts_of(at_place(place + 2 * step))
                        wanted = experts_of(at_place(place + step)) + (far[split:] if i else far[:split])
                        pk_s[i] = pack(1 + slot, wanted, recv_x[slot])
                        pack_copy(i).start()
            elif d == half - 1:
                for i in range(2):
                    pack_copy(i).wait_recv()
                    far_copy(i).start()
            else:
                for i in range(2):
                    far_copy(i).wait_recv()
            for i in range(2 if d < half else 1):
                s = 2 * d - 1 + i
                slot = s - 1
                if d <= half - 2:
                    stage_a(s, lambda j, slot=slot: pack(1 + slot, [me * local + j], recv_x[slot]))
                elif d == half - 1:
                    stage_a(s, stored(pk_r, i))
                else:
                    stage_a(s, lambda j: far_r[j // split, pl.ds(j % split * cap, cap), :])
                stage_b(s - 1)
                if s >= 2:
                    stage_c(s - 2, s == 2)
    else:
        send_x[1] = pack(0, experts_of(sender(1)), xn[...])

        @pl.loop(2, n)
        def _(s):
            send_x[s] = pack(0, experts_of(sender(s)), xn[...])
            x_copy(s - 1).start()

        for load in loads:
            load.wait()
        stage_a(0, own_rows)
        x_copy(n - 1).start()
        x_copy(1).wait_recv()
        stage_a(1, stored(recv_x, 1))
        stage_b(0)
        x_copy(2).wait_recv()
        stage_a(2, stored(recv_x, 2))
        stage_b(1)
        stage_c(0, True)

        @pl.loop(3, n)
        def _(s):
            x_copy(s).wait_recv()
            stage_a(s, stored(recv_x, s))
            stage_b(s - 1)
            stage_c(s - 2, False)

    stage_b(n - 1)
    stage_c(n - 2, False)
    acc[...] = combine(0)
    stage_c(n - 1, False)

    @pl.loop(1, n)
    def _(s):
        o_copy(s).wait_recv()
        acc[...] += combine(s)

    summed = acc[...]
    start_sum(1, jnp.sum(summed * summed, axis=1, keepdims=True))

    @pl.loop(0, n)
    def _(s):
        for o in range(1, nt):
            p_copy(s, o).wait_send()
            h_copy(s, o).wait_send()

    send_sum(1)

    @pl.loop(1, n)
    def _(s):
        o_copy(s).wait_send()

    if ring:
        for i in range(2):
            for d in range(1, half - 1):
                meta_copy(d, i).wait_send()
                for k in range(2):
                    block_copy(d, i, k).wait_send()
            pack_copy(i).wait_send()
            far_copy(i).wait_send()
    else:
        @pl.loop(1, n)
        def _(s):
            x_copy(s).wait_send()

    scale = finish_sum(1)
    out_ref[...] = (acc[...] * scale * last_gain_ref[...]).astype(BF)
    for k in range(2):
        for o in range(1, nt):
            sq_copy(k, o).wait_send()


def line_kernel(
    n, nt, local, cap, full, parts,
    x_ref, meta_ref, gain_ref, last_gain_ref, gate_hbm, up_hbm, down_hbm, out_ref,
    gate_v, up_v, down_v, xs, notes, scale_s, tri, cols, pick, lift, rows_o, pk_s, pk_r,
    part, recv_p, hid, out_o, ret_s, ret_r, comb, sum_s, sum_r, acc, sq, sq2,
    w_sem, own_sem, rel_sem, blk_sem, nown_sem, nrel_sem, note_sem, ks_sem, kr_sem,
    ps_sem, pr_sem, hs_sem, hr_sem, ts_sem, tr_sem, ss_sem, sr_sem, qs_sem, qr_sem,
):
    me = lax.axis_index("ep")
    my_tp = lax.axis_index("tp")
    ff = gate_v.shape[2]
    fq = ff // nt
    rows_all, width = x_ref.shape
    cw = width // parts
    count = local * cap
    last = n // 2 - 1
    z, side = me // 2, me % 2
    low = z <= last // 2
    inner = (z >= 1) & (z <= last - 1)
    end = jnp.logical_not(inner)
    step_in = jnp.where(low, 2, -2)
    inward = {"ep": me + step_in, "tp": my_tp}
    outward = {"ep": jnp.where(inner, me - step_in, me + step_in), "tp": my_tp}
    mate = me + 1 - 2 * side
    across = {"ep": mate, "tp": my_tp}
    spare = last + 1

    def block(s):
        if s == 0:
            return z
        near = jnp.where(inner, 0, 1) if s == 1 else (last if s == 2 else last - 1)
        return jnp.where(low, near, last - near)

    loads = [
        pltpu.make_async_copy(src, dst, w_sem.at[i])
        for i, (src, dst) in enumerate(((gate_hbm, gate_v), (up_hbm, up_v), (down_hbm, down_v)))
    ]
    for load in loads:
        load.start()

    barrier = pltpu.get_barrier_semaphore()
    pl.semaphore_signal(barrier, inc=1, device_id=inward)
    pl.semaphore_signal(barrier, inc=1, device_id=across)

    @pl.when(inner)
    def _():
        pl.semaphore_signal(barrier, inc=1, device_id=outward)

    for o in range(1, nt):
        pl.semaphore_signal(barrier, inc=1, device_id={"ep": me, "tp": lax.rem(my_tp + o, nt)})

    def col(c):
        return pl.ds(c * cw, cw)

    def dcol(c):
        return pl.ds(pl.multiple_of(c * cw, cw), cw)

    def eye():
        shape = (rows_all, rows_all)
        return lax.broadcasted_iota(jnp.int32, shape, 0) == lax.broadcasted_iota(jnp.int32, shape, 1)

    def sq_copy(k, o):
        q = lax.rem(my_tp + o, nt)
        return pltpu.make_async_remote_copy(
            sq.at[k], sq2.at[k, o - 1], qs_sem.at[k, o - 1], qr_sem.at[k, o - 1],
            device_id={"ep": me, "tp": q},
        )

    def start_sum(k, column):
        row = jnp.sum(jnp.where(eye(), column, 0.0), axis=0, keepdims=True)
        sq[k] = jnp.broadcast_to(row, sq.shape[1:])

    def send_sum(k):
        for o in range(1, nt):
            sq_copy(k, o).start()

    def finish_sum(k):
        for o in range(1, nt):
            sq_copy(k, o).wait_recv()
        total = sq[k]
        for o in range(1, nt):
            total = total + sq2[k, o - 1]
        return lax.rsqrt(total / full + EPSILON)

    def own_copy(d, c):
        return pltpu.make_async_remote_copy(
            x_ref.at[:, col(c)], xs.at[z, :, col(c)], own_sem.at[d, c], blk_sem.at[z, c],
            device_id=outward if d else inward,
        )

    def relay(s, c):
        b = block(s)
        return pltpu.make_async_remote_copy(
            xs.at[b, :, col(c)], xs.at[b, :, col(c)], rel_sem.at[s - 1, c], blk_sem.at[b, c],
            device_id=inward if s == 1 else outward,
        )

    def own_note(k, d):
        return pltpu.make_async_remote_copy(
            scale_s if k else meta_ref, notes.at[k, z], nown_sem.at[k, d], note_sem.at[k, z],
            device_id=outward if d else inward,
        )

    def relay_note(k, s):
        b = block(s)
        return pltpu.make_async_remote_copy(
            notes.at[k, b], notes.at[k, b], nrel_sem.at[k, s - 1], note_sem.at[k, b],
            device_id=inward if s == 1 else outward,
        )

    def pack_copy(s, c):
        return pltpu.make_async_remote_copy(
            pk_s.at[s, :, col(c)], pk_r.at[s, :, col(c)], ks_sem.at[s, c], kr_sem.at[s, c],
            device_id=across,
        )

    def ret_copy(s, c, at):
        return pltpu.make_async_remote_copy(
            ret_s.at[s, :, at(c)], ret_r.at[s, :, at(c)], ts_sem.at[s, c], tr_sem.at[s, c],
            device_id=across,
        )

    def sum_copy(s, c, at):
        slot = jnp.where(end, spare, block(s)) if s == 1 else block(s)
        ep = jnp.where(inner, outward["ep"], inward["ep"]) if s == 1 else inward["ep"]
        return pltpu.make_async_remote_copy(
            sum_s.at[s - 1, :, at(c)], sum_r.at[slot, :, at(c)], ss_sem.at[s - 1, c], sr_sem.at[slot, c],
            device_id={"ep": ep, "tp": my_tp},
        )

    def sum_wait(slot, c, at):
        pltpu.make_async_remote_copy(
            sum_s.at[0, :, at(c)], sum_r.at[slot, :, at(c)], ss_sem.at[0, c], sr_sem.at[slot, c],
            device_id=inward,
        ).wait_recv()

    def p_copy(i, o):
        q = lax.rem(my_tp + o, nt)
        return pltpu.make_async_remote_copy(
            part.at[i, q], recv_p.at[i, o - 1], ps_sem.at[i, o - 1], pr_sem.at[i, o - 1],
            device_id={"ep": me, "tp": q},
        )

    def h_copy(i, o, back=False):
        mine = lax.rem(my_tp - o + nt, nt) if back else my_tp
        q = lax.rem(my_tp - o + nt, nt) if back else lax.rem(my_tp + o, nt)
        return pltpu.make_async_remote_copy(
            hid.at[i, mine], hid.at[i, mine], hs_sem.at[i, o - 1], hr_sem.at[i, o - 1],
            device_id={"ep": me, "tp": q},
        )

    def prepare(s, meta, scale):
        row = lax.broadcasted_iota(jnp.int32, (16, rows_all), 0)
        name = jnp.where(row < local, me * local + row, mate * local + row - local)
        name = jnp.where(row < 2 * local, name, -1).astype(F32)
        first, second = meta[0:1] == name, meta[1:2] == name
        hit = first | second
        before = dot(jnp.where(hit, 1.0, 0.0).astype(BF), tri[...])
        rank = jnp.where(hit, before, -1.0)
        weight = jnp.where(first, meta[2:3], 0.0) + jnp.where(second, meta[3:4], 0.0)
        blank = jnp.zeros((128 - 32, rows_all), F32)
        cols[s] = jnp.concatenate([rank, weight, blank], axis=0).T
        spot = lax.broadcasted_iota(jnp.int32, (cap, rows_all), 0).astype(F32)
        for e in range(2 * local):
            at = pl.ds(e * cap, cap)
            here = spot == rank[e:e + 1]
            pick[at, :] = jnp.where(here, 1.0, 0.0).astype(BF)
            total = jnp.sum(jnp.where(here, scale[0:1], 0.0), axis=1, keepdims=True)
            lift[at, :] = jnp.broadcast_to(total, (cap, lift.shape[1]))

    def pack(s, c):
        values = x_ref[:, col(c)] if s == 0 else xs[block(s), :, col(c)]
        gain = gain_ref[:, col(c)]
        far = dot(pick[pl.ds(count, count), :], values) * lift[pl.ds(count, count), 0:1] * gain
        pk_s[s, :, col(c)] = far.astype(BF)
        pack_copy(s, c).start()
        near = dot(pick[pl.ds(0, count), :], values) * lift[pl.ds(0, count), 0:1] * gain
        rows_o[:, col(c)] = near.astype(BF)

    def stage_a(s, h):
        i = 2 * s + h
        if h:
            for c in range(parts):
                pack_copy(s, c).wait_recv()
        for j in range(local):
            at = pl.ds(j * cap, cap)
            rows = pk_r[s, at, :] if h else rows_o[at, :]
            gate = dot(rows, gate_v[j]).astype(BF)
            upper = dot(rows, up_v[j]).astype(BF)
            for q in range(nt):
                part[i, q, at, pl.ds(0, fq)] = gate[:, q * fq:(q + 1) * fq]
                part[i, q, at, pl.ds(fq, fq)] = upper[:, q * fq:(q + 1) * fq]
        for o in range(1, nt):
            p_copy(i, o).start()

    def stage_b(s, h):
        i = 2 * s + h
        for o in range(1, nt):
            p_copy(i, o).wait_recv()
        total = part[i, my_tp].astype(F32)
        for o in range(1, nt):
            total = total + recv_p[i, o - 1].astype(F32)
        gate, upper = total[:, :fq], total[:, fq:]
        hid[i, my_tp] = (gate / (1.0 + jnp.exp(-gate)) * upper).astype(BF)
        for o in range(1, nt):
            h_copy(i, o).start()

    def stage_c(s, h):
        i = 2 * s + h
        for o in range(1, nt):
            h_copy(i, o, True).wait_recv()
        hidden = [
            jnp.concatenate([hid[i, q, pl.ds(j * cap, cap), :] for q in range(nt)], axis=1)
            for j in range(local)
        ]
        for c in range(parts if h else 1):
            piece = col(c) if h else pl.ds(0, width)
            target = ret_s if h else out_o
            for j in range(local):
                target[s, pl.ds(j * cap, cap), piece] = dot(hidden[j], down_v[j, :, piece]).astype(BF)
            if h:
                ret_copy(s, c, col).start()

    def weave(s):
        table = cols[s]
        spot = lax.broadcasted_iota(jnp.int32, (rows_all, cap), 1).astype(F32)
        for e in range(2 * local):
            here = spot == table[:, e:e + 1]
            comb[:, pl.ds(e * cap, cap)] = jnp.where(here, table[:, 16 + e:17 + e], 0.0).astype(BF)

    def mix(s, c):
        ret_copy(s, c, dcol).wait_recv()
        near = dot(comb[:, pl.ds(0, count)], out_o[s, :, dcol(c)])
        return near + dot(comb[:, pl.ds(count, count)], ret_r[s, :, dcol(c)])

    def stage_d(s, more):
        weave(s)

        @pl.loop(0, parts)
        def _(c):
            total = mix(s, c)
            if more:
                sum_wait(block(s), c, dcol)
                total = total + sum_r[block(s), :, dcol(c)].astype(F32)
            sum_s[s - 1, :, dcol(c)] = total.astype(BF)
            sum_copy(s, c, dcol).start()

    def heads(lead):
        for c in lead:
            own_copy(0, c).start()

            @pl.when(inner)
            def _(c=c):
                own_copy(1, c).start()

    def send_note(k):
        own_note(k, 0).start()

        @pl.when(inner)
        def _():
            own_note(k, 1).start()

    def take_notes(s):
        for k in range(2):
            relay_note(k, s).wait_recv()

            @pl.when(inner)
            def _(k=k):
                relay_note(k, s).start()

    half = parts // 2
    ahead = {}
    for c in range(parts):
        ahead[(1, c)] = [(1, c)]
    for c in range(parts):
        spot = parts - half + c
        ahead.setdefault((1 + spot // parts, spot % parts), []).append((2, c))
    for c in range(parts):
        spot = parts + half - 1 + max(c - half + 1, 0)
        ahead.setdefault((1 + spot // parts, spot % parts), []).append((3, c))

    def arrive(s, c):
        @pl.when(inner)
        def _():
            for item in ahead.get((s, c), ()):
                relay(*item).wait_recv()
                relay(*item).start()
            if (s, c) == (1, parts - 1):
                for k in range(half, parts):
                    own_copy(0, k).start()

        @pl.when(end)
        def _():
            relay(s, c).wait_recv()

    pl.semaphore_wait(barrier, jnp.where(inner, 3, 2) + nt - 1)
    send_note(0)
    heads(range(half))
    values = x_ref[...].astype(F32)
    start_sum(0, jnp.sum(values * values, axis=1, keepdims=True))
    send_sum(0)
    shape = (rows_all, rows_all)
    earlier = lax.broadcasted_iota(jnp.int32, shape, 0) < lax.broadcasted_iota(jnp.int32, shape, 1)
    tri[...] = jnp.where(earlier, 1.0, 0.0).astype(BF)
    scale_s[...] = finish_sum(0)
    send_note(1)
    for c in range(half, parts):
        @pl.when(end)
        def _(c=c):
            own_copy(0, c).start()

        @pl.when(inner)
        def _(c=c):
            own_copy(1, c).start()

    prepare(0, meta_ref[...], scale_s[...])
    for c in range(parts):
        pack(0, c)
    for load in loads:
        load.wait()
    stage_a(0, 0)

    for s in range(1, last + 1):
        take_notes(s)
        prepare(s, notes[0, block(s)], notes[1, block(s)])
        for c in range(parts):
            arrive(s, c)
            pack(s, c)
            if c == 0:
                stage_a(s - 1, 1)
                stage_b(s - 1, 0)
            elif c == 1:
                stage_b(s - 1, 1)
                stage_c(s - 1, 0)
            elif c == 2:
                stage_c(s - 1, 1)
        stage_a(s, 0)
        if s >= 2:
            @pl.when(end)
            def _(s=s):
                stage_d(s - 1, False)

    stage_a(last, 1)
    stage_b(last, 0)
    stage_b(last, 1)
    stage_c(last, 0)
    stage_c(last, 1)

    @pl.when(end)
    def _():
        stage_d(last, False)

    @pl.when(inner)
    def _():
        stage_d(2, True)
        stage_d(1, True)
        stage_d(3, True)

    weave(0)

    @pl.loop(0, parts)
    def _(c):
        acc[:, dcol(c)] = mix(0, c)

    @pl.when(inner)
    def _():
        @pl.loop(0, parts)
        def _(c):
            sum_wait(spare, c, dcol)
            acc[:, dcol(c)] += sum_r[spare, :, dcol(c)].astype(F32)

    @pl.loop(0, parts)
    def _(c):
        sum_wait(z, c, dcol)
        acc[:, dcol(c)] += sum_r[z, :, dcol(c)].astype(F32)

    summed = acc[...]
    start_sum(1, jnp.sum(summed * summed, axis=1, keepdims=True))
    send_sum(1)

    for i in range(2 * last + 2):
        for o in range(1, nt):
            p_copy(i, o).wait_send()
            h_copy(i, o).wait_send()
    for s in range(last + 1):
        for c in range(parts):
            pack_copy(s, c).wait_send()
            ret_copy(s, c, col).wait_send()
            if s:
                sum_copy(s, c, col).wait_send()
    for c in range(parts):
        own_copy(0, c).wait_send()
    for k in range(2):
        own_note(k, 0).wait_send()

    @pl.when(inner)
    def _():
        for c in range(parts):
            own_copy(1, c).wait_send()
            for s in range(1, last + 1):
                relay(s, c).wait_send()
        for k in range(2):
            own_note(k, 1).wait_send()
            for s in range(1, last + 1):
                relay_note(k, s).wait_send()

    scale = jnp.sum(jnp.where(eye(), finish_sum(1)[0:1], 0.0), axis=1, keepdims=True)
    out_ref[...] = (acc[...] * scale * last_gain_ref[...]).astype(BF)
    for k in range(2):
        for o in range(1, nt):
            sq_copy(k, o).wait_send()


def line_call(n, nt, local, cap, full, tokens, meta, norm_gain, gate_weight, up_weight, down_weight, final_gain):
    rows, width = tokens.shape
    ff = gate_weight.shape[2]
    line = n // 2
    count = local * cap
    parts = 4
    any_spec = pl.BlockSpec(memory_space=pl.ANY)
    vmem = pl.BlockSpec(memory_space=pltpu.VMEM)
    dma = pltpu.SemaphoreType.DMA
    return pl.pallas_call(
        functools.partial(line_kernel, n, nt, local, cap, full, parts),
        out_shape=jax.ShapeDtypeStruct((rows, width), BF),
        in_specs=[vmem, vmem, vmem, vmem, any_spec, any_spec, any_spec],
        out_specs=vmem,
        scratch_shapes=[
            pltpu.VMEM(gate_weight.shape, BF),
            pltpu.VMEM(up_weight.shape, BF),
            pltpu.VMEM(down_weight.shape, BF),
            pltpu.VMEM((line, rows, width), BF),
            pltpu.VMEM((2, line, 8, rows), F32),
            pltpu.VMEM((8, rows), F32),
            pltpu.VMEM((rows, rows), BF),
            pltpu.VMEM((line, rows, 128), F32),
            pltpu.VMEM((2 * count, rows), BF),
            pltpu.VMEM((2 * count, 128), F32),
            pltpu.VMEM((count, width), BF),
            pltpu.VMEM((line, count, width), BF),
            pltpu.VMEM((line, count, width), BF),
            pltpu.VMEM((n, nt, count, 2 * ff // nt), BF),
            pltpu.VMEM((n, nt - 1, count, 2 * ff // nt), BF),
            pltpu.VMEM((n, nt, count, ff // nt), BF),
            pltpu.VMEM((line, count, width), BF),
            pltpu.VMEM((line, count, width), BF),
            pltpu.VMEM((line, count, width), BF),
            pltpu.VMEM((rows, 2 * count), BF),
            pltpu.VMEM((line - 1, rows, width), BF),
            pltpu.VMEM((line + 1, rows, width), BF),
            pltpu.VMEM((rows, width), F32),
            pltpu.VMEM((2, 8, rows), F32),
            pltpu.VMEM((2, nt - 1, 8, rows), F32),
            dma((3,)),
            dma((2, parts)),
            dma((line - 1, parts)),
            dma((line, parts)),
            dma((2, 2)),
            dma((2, line - 1)),
            dma((2, line)),
            dma((line, parts)),
            dma((line, parts)),
            dma((n, nt - 1)),
            dma((n, nt - 1)),
            dma((n, nt - 1)),
            dma((n, nt - 1)),
            dma((line, parts)),
            dma((line, parts)),
            dma((line - 1, parts)),
            dma((line + 1, parts)),
            dma((2, nt - 1)),
            dma((2, nt - 1)),
        ],
        compiler_params=pltpu.CompilerParams(
            collective_id=0, has_side_effects=True, vmem_limit_bytes=62 * 1024 * 1024
        ),
    )(tokens, meta, norm_gain[None], final_gain[None], gate_weight, up_weight, down_weight)


RING_BYTES = 24 * 1024 * 1024


def body(tokens, routes, route_weights, norm_gain, gate_weight, up_weight, down_weight, final_gain):
    n, nt = lax.axis_size("ep"), lax.axis_size("tp")
    local, width, ff = gate_weight.shape
    experts = n * local
    rows = tokens.shape[0]
    full = width * nt
    cap = 4 * rows // experts
    count = local * cap
    blocks = max(n - 4, 0)
    ring = n % 2 == 0 and n >= 6 and local % 2 == 0 and blocks * rows * width * 2 <= RING_BYTES
    meta = jnp.concatenate(
        [routes.T.astype(F32), route_weights.T, jnp.zeros((4, rows), F32)], axis=0
    )
    if n == 8 and local <= 8 and width % 512 == 0 and cap % 128 == 0:
        return line_call(
            n, nt, local, cap, full, tokens, meta, norm_gain, gate_weight, up_weight, down_weight, final_gain
        )
    tables = 1 + blocks if ring else 1
    packed = count + local // 2 * cap

    any_spec = pl.BlockSpec(memory_space=pl.ANY)
    vmem = pl.BlockSpec(memory_space=pltpu.VMEM)
    dma = pltpu.SemaphoreType.DMA

    def only(ring_shape, shape, kind=BF):
        return pltpu.VMEM(ring_shape if ring else shape, kind)

    tiny = (1, 16, 128)
    return pl.pallas_call(
        functools.partial(kernel, n, nt, local, cap, ring, full),
        out_shape=jax.ShapeDtypeStruct((rows, width), BF),
        in_specs=[vmem, vmem, vmem, vmem, any_spec, any_spec, any_spec],
        out_specs=vmem,
        scratch_shapes=[
            pltpu.VMEM(gate_weight.shape, BF),
            pltpu.VMEM(up_weight.shape, BF),
            pltpu.VMEM(down_weight.shape, BF),
            pltpu.VMEM((rows, width), BF),
            pltpu.VMEM((rows, width), F32),
            pltpu.VMEM((rows, rows), BF),
            pltpu.VMEM((tables, experts, rows), F32),
            pltpu.VMEM((tables, experts, rows), F32),
            pltpu.VMEM((2, 8, rows), F32),
            pltpu.VMEM((2, nt - 1, 8, rows), F32),
            only(tiny, (n, count, width)),
            only((blocks, rows, width), (n, count, width)),
            only((2, packed, width), tiny),
            only((2, packed, width), tiny),
            only((2, local // 2 * cap, width), tiny),
            only((blocks, 8, rows), (1, 8, 128), F32),
            pltpu.VMEM((n, nt, count, 2 * ff // nt), BF),
            pltpu.VMEM((n, nt - 1, count, 2 * ff // nt), BF),
            pltpu.VMEM((n, nt, count, ff // nt), BF),
            pltpu.VMEM((n, count, width), BF),
            pltpu.VMEM((n, count, width), BF),
            dma((3,)),
            dma((blocks, 2) if ring else (n,)),
            dma((blocks, 2) if ring else (n,)),
            dma((2,)),
            dma((2,)),
            dma((2,)),
            dma((2,)),
            dma((blocks,) if ring else (1,)),
            dma((blocks,) if ring else (1,)),
            dma((n, nt - 1)),
            dma((n, nt - 1)),
            dma((n, nt - 1)),
            dma((n, nt - 1)),
            dma((n,)),
            dma((n,)),
            dma((2, nt - 1)),
            dma((2, nt - 1)),
        ],
        compiler_params=pltpu.CompilerParams(
            collective_id=0, has_side_effects=True, vmem_limit_bytes=60 * 1024 * 1024
        ),
    )(tokens, meta, norm_gain[None], final_gain[None], gate_weight, up_weight, down_weight)


def solution(mesh):
    in_specs = (
        P("ep", "tp"),
        P("ep", None),
        P("ep", None),
        P("tp"),
        P("ep", "tp", None),
        P("ep", "tp", None),
        P("ep", None, "tp"),
        P("tp"),
    )
    return jax.shard_map(body, mesh=mesh, in_specs=in_specs, out_specs=P("ep", "tp"), check_vma=False)
```

```python
import functools

import jax
import jax.numpy as jnp
from jax import lax
from jax.experimental import pallas as pl
from jax.experimental.pallas import tpu as pltpu
from jax.sharding import PartitionSpec as P

EPSILON = 1e-06
BF = jnp.bfloat16
F32 = jnp.float32


def dot(a, b):
    return jnp.dot(a, b, preferred_element_type=F32)


def dot_t(a, b):
    return lax.dot_general(a, b, (((0,), (0,)), ((), ())), preferred_element_type=F32)


def kernel(
    n, nt, local, cap, ring, full,
    x_ref, meta_ref, gain_ref, last_gain_ref, gate_hbm, up_hbm, down_hbm, out_ref,
    gate_v, up_v, down_v, xn, acc, tri, rank_t, wt_t, sq, sq2,
    send_x, recv_x, pk_s, pk_r, far_r, meta_r,
    part, recv_p, hid, out_s, out_r,
    w_sem, xs_sem, xr_sem, ks_sem, kr_sem, fs_sem, fr_sem, ms_sem, mr_sem,
    ps_sem, pr_sem, hs_sem, hr_sem, os_sem, or_sem, qs_sem, qr_sem,
):
    me = lax.axis_index("ep")
    my_tp = lax.axis_index("tp")
    ff = gate_v.shape[2]
    fq = ff // nt
    rows_all = x_ref.shape[0]
    half = n // 2
    chunk = rows_all // 2
    count = local * cap
    split = local // 2

    loads = [
        pltpu.make_async_copy(src, dst, w_sem.at[i])
        for i, (src, dst) in enumerate(((gate_hbm, gate_v), (up_hbm, up_v), (down_hbm, down_v)))
    ]
    for load in loads:
        load.start()

    barrier = pltpu.get_barrier_semaphore()

    @pl.loop(1, n)
    def _(s):
        pl.semaphore_signal(barrier, inc=1, device_id={"ep": lax.rem(me + s, n), "tp": my_tp})

    for o in range(1, nt):
        pl.semaphore_signal(barrier, inc=1, device_id={"ep": me, "tp": lax.rem(my_tp + o, nt)})

    place = jnp.where(me % 2 == 0, me // 2, n - 1 - me // 2)

    def at_place(p):
        p = lax.rem(p + 2 * n, n)
        return jnp.where(p < half, 2 * p, 2 * (n - 1 - p) + 1)

    def shift(s):
        return (1 - 2 * ((s + 1) % 2)) * ((s + 1) // 2)

    def source(s):
        if ring:
            return at_place(place - shift(s))
        return lax.rem(me - s + n, n)

    def sender(s):
        if ring:
            return at_place(place + shift(s))
        return lax.rem(me + s, n)

    def eye():
        shape = (rows_all, rows_all)
        return lax.broadcasted_iota(jnp.int32, shape, 0) == lax.broadcasted_iota(jnp.int32, shape, 1)

    def sq_copy(k, o):
        q = lax.rem(my_tp + o, nt)
        return pltpu.make_async_remote_copy(
            sq.at[k], sq2.at[k, o - 1], qs_sem.at[k, o - 1], qr_sem.at[k, o - 1],
            device_id={"ep": me, "tp": q},
        )

    def start_sum(k, column):
        row = jnp.sum(jnp.where(eye(), column, 0.0), axis=0, keepdims=True)
        sq[k] = jnp.broadcast_to(row, sq.shape[1:])

    def send_sum(k):
        for o in range(1, nt):
            sq_copy(k, o).start()

    def finish_sum(k):
        for o in range(1, nt):
            sq_copy(k, o).wait_recv()
        total = sq[k]
        for o in range(1, nt):
            total = total + sq2[k, o - 1]
        scale = lax.rsqrt(total[0:1] / full + EPSILON)
        return jnp.sum(jnp.where(eye(), scale, 0.0), axis=1, keepdims=True)

    def make_table(slot, meta):
        names = lax.broadcasted_iota(jnp.int32, rank_t.shape[1:], 0).astype(F32)
        first, second = meta[0:1] == names, meta[1:2] == names
        hit = first | second
        before = dot(jnp.where(hit, 1.0, 0.0).astype(BF), tri[...])
        rank_t[slot] = jnp.where(hit, before, -1.0)
        wt_t[slot] = jnp.where(first, meta[2:3], 0.0) + jnp.where(second, meta[3:4], 0.0)

    def onehot(slot, expert, weighted=False):
        rank = rank_t[slot, pl.ds(expert, 1), :]
        hit = lax.broadcasted_iota(jnp.int32, (cap, rows_all), 0).astype(F32) == rank
        return jnp.where(hit, wt_t[slot, pl.ds(expert, 1), :] if weighted else F32(1.0), F32(0.0))

    def pack(slot, experts, block):
        pick = jnp.concatenate([onehot(slot, e) for e in experts], axis=0).astype(BF)
        return dot(pick, block).astype(BF)

    def experts_of(owner):
        return [owner * local + j for j in range(local)]

    def x_copy(s):
        return pltpu.make_async_remote_copy(
            send_x.at[s], recv_x.at[s], xs_sem.at[s], xr_sem.at[s],
            device_id={"ep": sender(s), "tp": my_tp},
        )

    def ahead(i):
        return {"ep": at_place(place + 1 - 2 * i), "tp": my_tp}

    def block_copy(d, i, k):
        piece = pl.ds(k * chunk, chunk)
        src = xn.at[piece] if d == 1 else recv_x.at[2 * d - 4 + i, piece]
        slot = 2 * d - 2 + i
        return pltpu.make_async_remote_copy(
            src, recv_x.at[slot, piece], xs_sem.at[slot, k], xr_sem.at[slot, k], device_id=ahead(i)
        )

    def meta_copy(d, i):
        slot = 2 * d - 2 + i
        return pltpu.make_async_remote_copy(
            meta_ref if d == 1 else meta_r.at[slot - 2], meta_r.at[slot],
            ms_sem.at[slot], mr_sem.at[slot], device_id=ahead(i),
        )

    def pack_copy(i):
        return pltpu.make_async_remote_copy(
            pk_s.at[i], pk_r.at[i], ks_sem.at[i], kr_sem.at[i], device_id=ahead(i)
        )

    def far_copy(i):
        return pltpu.make_async_remote_copy(
            pk_r.at[i, pl.ds(count, split * cap)], far_r.at[i], fs_sem.at[i], fr_sem.at[i],
            device_id=ahead(i),
        )

    def p_copy(s, o):
        q = lax.rem(my_tp + o, nt)
        return pltpu.make_async_remote_copy(
            part.at[s, q], recv_p.at[s, o - 1], ps_sem.at[s, o - 1], pr_sem.at[s, o - 1],
            device_id={"ep": me, "tp": q},
        )

    def h_copy(s, o, back=False):
        mine = lax.rem(my_tp - o + nt, nt) if back else my_tp
        q = lax.rem(my_tp - o + nt, nt) if back else lax.rem(my_tp + o, nt)
        return pltpu.make_async_remote_copy(
            hid.at[s, mine], hid.at[s, mine], hs_sem.at[s, o - 1], hr_sem.at[s, o - 1],
            device_id={"ep": me, "tp": q},
        )

    def o_copy(s):
        return pltpu.make_async_remote_copy(
            out_s.at[s], out_r.at[s], os_sem.at[s], or_sem.at[s],
            device_id={"ep": source(s), "tp": my_tp},
        )

    def stage_a(s, rows_of):
        for j in range(local):
            rows = rows_of(j)
            gate = dot(rows, gate_v[j]).astype(BF)
            upper = dot(rows, up_v[j]).astype(BF)
            for q in range(nt):
                part[s, q, pl.ds(j * cap, cap), pl.ds(0, fq)] = gate[:, q * fq:(q + 1) * fq]
                part[s, q, pl.ds(j * cap, cap), pl.ds(fq, fq)] = upper[:, q * fq:(q + 1) * fq]
        for o in range(1, nt):
            p_copy(s, o).start()

    def stage_b(s):
        for o in range(1, nt):
            p_copy(s, o).wait_recv()
        total = part[s, my_tp].astype(F32)
        for o in range(1, nt):
            total = total + recv_p[s, o - 1].astype(F32)
        gate, upper = total[:, :fq], total[:, fq:]
        hid[s, my_tp] = (gate / (1.0 + jnp.exp(-gate)) * upper).astype(BF)
        for o in range(1, nt):
            h_copy(s, o).start()

    def stage_c(s, own):
        for o in range(1, nt):
            h_copy(s, o, True).wait_recv()
        target = out_r if own else out_s
        for j in range(local):
            hidden = jnp.concatenate([hid[s, q, pl.ds(j * cap, cap), :] for q in range(nt)], axis=1)
            target[s, pl.ds(j * cap, cap), :] = dot(hidden, down_v[j]).astype(BF)
        if not own:
            o_copy(s).start()

    def combine(s):
        weight = jnp.concatenate([onehot(0, e, True) for e in experts_of(sender(s))], axis=0)
        high = weight.astype(BF)
        low = (weight - high.astype(F32)).astype(BF)
        rows = out_r[s]
        return dot_t(high, rows) + dot_t(low, rows)

    values = x_ref[...].astype(F32)
    start_sum(0, jnp.sum(values * values, axis=1, keepdims=True))
    shape = (rows_all, rows_all)
    earlier = lax.broadcasted_iota(jnp.int32, shape, 0) < lax.broadcasted_iota(jnp.int32, shape, 1)
    tri[...] = jnp.where(earlier, 1.0, 0.0).astype(BF)
    pl.semaphore_wait(barrier, n - 1 + nt - 1)
    send_sum(0)
    if ring:
        for i in range(2):
            meta_copy(1, i).start()
    make_table(0, meta_ref[...])
    scale = finish_sum(0)
    xn[...] = (x_ref[...].astype(F32) * scale * gain_ref[...]).astype(BF)

    def own_rows(j):
        return pack(0, [me * local + j], xn[...])

    def stored(ref, slot):
        return lambda j: ref[slot, pl.ds(j * cap, cap), :]

    if ring:
        for k in range(2):
            for i in range(2):
                block_copy(1, i, k).start()
        for load in loads:
            load.wait()
        stage_a(0, own_rows)
        for d in range(1, half + 1):
            if d <= half - 2:
                for k in range(2):
                    for i in range(2):
                        block_copy(d, i, k).wait_recv()
                        if d < half - 2:
                            block_copy(d + 1, i, k).start()
                for i in range(2):
                    slot = 2 * d - 2 + i
                    meta_copy(d, i).wait_recv()
                    if d < half - 2:
                        meta_copy(d + 1, i).start()
                    make_table(1 + slot, meta_r[slot])
                if d == half - 2:
                    for i in range(2):
                        slot = 2 * d - 2 + i
                        step = 1 - 2 * i
                        far = experts_of(at_place(place + 2 * step))
                        wanted = experts_of(at_place(place + step)) + (far[split:] if i else far[:split])
                        pk_s[i] = pack(1 + slot, wanted, recv_x[slot])
                        pack_copy(i).start()
            elif d == half - 1:
                for i in range(2):
                    pack_copy(i).wait_recv()
                    far_copy(i).start()
            else:
                for i in range(2):
                    far_copy(i).wait_recv()
            for i in range(2 if d < half else 1):
                s = 2 * d - 1 + i
                slot = s - 1
                if d <= half - 2:
                    stage_a(s, lambda j, slot=slot: pack(1 + slot, [me * local + j], recv_x[slot]))
                elif d == half - 1:
                    stage_a(s, stored(pk_r, i))
                else:
                    stage_a(s, lambda j: far_r[j // split, pl.ds(j % split * cap, cap), :])
                stage_b(s - 1)
                if s >= 2:
                    stage_c(s - 2, s == 2)
    else:
        send_x[1] = pack(0, experts_of(sender(1)), xn[...])

        @pl.loop(2, n)
        def _(s):
            send_x[s] = pack(0, experts_of(sender(s)), xn[...])
            x_copy(s - 1).start()

        for load in loads:
            load.wait()
        stage_a(0, own_rows)
        x_copy(n - 1).start()
        x_copy(1).wait_recv()
        stage_a(1, stored(recv_x, 1))
        stage_b(0)
        x_copy(2).wait_recv()
        stage_a(2, stored(recv_x, 2))
        stage_b(1)
        stage_c(0, True)

        @pl.loop(3, n)
        def _(s):
            x_copy(s).wait_recv()
            stage_a(s, stored(recv_x, s))
            stage_b(s - 1)
            stage_c(s - 2, False)

    stage_b(n - 1)
    stage_c(n - 2, False)
    acc[...] = combine(0)
    stage_c(n - 1, False)

    @pl.loop(1, n)
    def _(s):
        o_copy(s).wait_recv()
        acc[...] += combine(s)

    summed = acc[...]
    start_sum(1, jnp.sum(summed * summed, axis=1, keepdims=True))

    @pl.loop(0, n)
    def _(s):
        for o in range(1, nt):
            p_copy(s, o).wait_send()
            h_copy(s, o).wait_send()

    send_sum(1)

    @pl.loop(1, n)
    def _(s):
        o_copy(s).wait_send()

    if ring:
        for i in range(2):
            for d in range(1, half - 1):
                meta_copy(d, i).wait_send()
                for k in range(2):
                    block_copy(d, i, k).wait_send()
            pack_copy(i).wait_send()
            far_copy(i).wait_send()
    else:
        @pl.loop(1, n)
        def _(s):
            x_copy(s).wait_send()

    scale = finish_sum(1)
    out_ref[...] = (acc[...] * scale * last_gain_ref[...]).astype(BF)
    for k in range(2):
        for o in range(1, nt):
            sq_copy(k, o).wait_send()


END_ORDER = (
    ("a", 0, 0), ("weave", 0), ("prep", 1), ("weave", 1), ("b", 0, 0), ("pack", 1, 0), ("a", 0, 1), ("pack",
    1, 1), ("c", 0), ("pack", 1, 2), ("pack", 1, 3), ("a", 1, 0), ("prep", 2), ("weave", 2), ("pack", 2, 0),
    ("a", 1, 1), ("pack", 2, 1), ("b", 1, 0), ("b", 0, 1), ("pack", 2, 2), ("c", 1), ("b", 1, 1), ("c1", 0,
    0), ("pack", 2, 3), ("a", 2, 0), ("prep", 3), ("weave", 3), ("mix0", 0), ("c1", 1, 0), ("pack", 3, 0),
    ("a", 2, 1), ("d", 1, 0), ("c1", 1, 1), ("pack", 3, 1), ("b", 2, 0), ("d", 1, 1), ("c1", 1, 2), ("b", 2,
    1), ("pack", 3, 2), ("c", 2), ("d", 1, 2), ("c1", 1, 3), ("pack", 3, 3), ("a", 3, 0), ("d", 1, 3), ("c1",
    2, 0), ("c1", 2, 1), ("a", 3, 1), ("d", 2, 0), ("c1", 2, 2), ("d", 2, 1), ("c1", 2, 3), ("b", 3, 0), ("d",
    2, 2), ("c1", 0, 1), ("b", 3, 1), ("d", 2, 3), ("c1", 0, 2), ("c", 3), ("mix0", 1), ("c1", 0, 3), ("mix0",
    2), ("c1", 3, 0), ("mix0", 3), ("c1", 3, 1), ("d", 3, 0), ("c1", 3, 2), ("d", 3, 1), ("c1", 3, 3),
    ("last", 0), ("d", 3, 2), ("d", 3, 3), ("last", 1), ("last", 2), ("last", 3),
)

INNER_ORDER = (
    ("a", 0, 0), ("passn", 1), ("passn", 3), ("pass", 1, 0), ("prep", 1), ("weave", 1), ("weave", 0), ("pass",
    1, 1), ("passn", 2), ("b", 0, 0), ("pack", 1, 0), ("a", 0, 1), ("pack", 1, 1), ("pass", 1, 2), ("pass", 2,
    0), ("c", 0), ("pack", 1, 2), ("pass", 1, 3), ("pack", 1, 3), ("a", 1, 0), ("prep", 2), ("weave", 2),
    ("pass", 2, 1), ("ownin", 2), ("ownin", 3), ("pack", 2, 0), ("pack", 2, 1), ("pass", 2, 2), ("b", 0, 1),
    ("pack", 2, 2), ("b", 1, 0), ("pass", 2, 3), ("pack", 2, 3), ("pass", 3, 0), ("pass", 3, 1), ("a", 1, 1),
    ("prep", 3), ("weave", 3), ("c1", 0, 0), ("c", 1), ("c1", 0, 1), ("pass", 3, 2), ("a", 2, 1), ("mix0", 0),
    ("c1", 0, 2), ("mix0", 1), ("c1", 0, 3), ("pass", 3, 3), ("b", 1, 1), ("mix0", 2), ("b", 2, 1), ("mix0",
    3), ("c1", 1, 0), ("a", 2, 0), ("pack", 3, 0), ("pack", 3, 1), ("pack", 3, 2), ("b", 2, 0), ("spare", 0),
    ("pack", 3, 3), ("a", 3, 0), ("c", 2), ("c1", 1, 1), ("spare", 1), ("c1", 1, 2), ("a", 3, 1), ("c1", 1,
    3), ("spare", 2), ("c1", 2, 0), ("b", 3, 0), ("c1", 2, 1), ("b", 3, 1), ("spare", 3), ("c1", 2, 2), ("c",
    3), ("c1", 2, 3), ("d", 2, 0), ("c1", 3, 0), ("c1", 3, 1), ("d", 2, 1), ("c1", 3, 2), ("d", 1, 0), ("c1",
    3, 3), ("d", 2, 2), ("d", 1, 1), ("d", 2, 3), ("d", 1, 2), ("d", 3, 0), ("d", 1, 3), ("d", 3, 1), ("last",
    0), ("d", 3, 2), ("last", 1), ("d", 3, 3), ("last", 2), ("last", 3),
)


def line_kernel(
    n, nt, local, cap, full, parts,
    x_hbm, route_ref, weight_ref, gain_ref, last_gain_ref, gate_hbm, up_hbm, down_hbm, out_ref,
    gate_v, up_v, down_v, x_ref, xs, notes, note_s, tri, cols, pick, lift, pk_s, pk_r,
    part, recv_p, hid, out_o, ret_s, ret_r, comb, sum_s, sum_r, acc, sq, sq2,
    w_sem, x_sem, own_sem, rel_sem, blk_sem, nown_sem, nrel_sem, note_sem, ks_sem, kr_sem,
    ps_sem, pr_sem, hs_sem, hr_sem, ts_sem, tr_sem, ss_sem, sr_sem, qs_sem, qr_sem,
):
    me = lax.axis_index("ep")
    my_tp = lax.axis_index("tp")
    ff = gate_v.shape[2]
    fq = ff // nt
    rows_all, width = x_ref.shape
    cw = width // parts
    count = local * cap
    last = n // 2 - 1
    z, side = me // 2, me % 2
    low = z <= last // 2
    inner = (z >= 1) & (z <= last - 1)
    end = jnp.logical_not(inner)
    step_in = jnp.where(low, 2, -2)
    inward = {"ep": me + step_in, "tp": my_tp}
    outward = {"ep": jnp.where(inner, me - step_in, me + step_in), "tp": my_tp}
    mate = me + 1 - 2 * side
    across = {"ep": mate, "tp": my_tp}
    spare = last + 1

    def block(s):
        if s == 0:
            return z
        near = jnp.where(inner, 0, 1) if s == 1 else (last if s == 2 else last - 1)
        return jnp.where(low, near, last - near)

    loads = [
        pltpu.make_async_copy(src, dst, w_sem.at[i])
        for i, (src, dst) in enumerate(((gate_hbm, gate_v), (up_hbm, up_v), (down_hbm, down_v)))
    ]
    x_loads = [
        pltpu.make_async_copy(x_hbm.at[:, pl.ds(c * cw, cw)], x_ref.at[:, pl.ds(c * cw, cw)], x_sem.at[c])
        for c in range(parts)
    ]
    for load in x_loads + loads:
        load.start()

    barrier = pltpu.get_barrier_semaphore()
    pl.semaphore_signal(barrier, inc=1, device_id=inward)
    pl.semaphore_signal(barrier, inc=1, device_id=across)

    @pl.when(inner)
    def _():
        pl.semaphore_signal(barrier, inc=1, device_id=outward)

    for o in range(1, nt):
        pl.semaphore_signal(barrier, inc=1, device_id={"ep": me, "tp": lax.rem(my_tp + o, nt)})

    def col(c):
        return pl.ds(c * cw, cw)

    def dcol(c):
        return pl.ds(pl.multiple_of(c * cw, cw), cw)

    def eye():
        shape = (rows_all, rows_all)
        return lax.broadcasted_iota(jnp.int32, shape, 0) == lax.broadcasted_iota(jnp.int32, shape, 1)

    def sq_copy(k, o):
        q = lax.rem(my_tp + o, nt)
        return pltpu.make_async_remote_copy(
            sq.at[k], sq2.at[k, o - 1], qs_sem.at[k, o - 1], qr_sem.at[k, o - 1],
            device_id={"ep": me, "tp": q},
        )

    def start_sum(k, column):
        row = jnp.sum(jnp.where(eye(), column, 0.0), axis=0, keepdims=True)
        sq[k] = jnp.broadcast_to(row, sq.shape[1:])

    def send_sum(k):
        for o in range(1, nt):
            sq_copy(k, o).start()

    def finish_sum(k):
        for o in range(1, nt):
            sq_copy(k, o).wait_recv()
        total = sq[k]
        for o in range(1, nt):
            total = total + sq2[k, o - 1]
        return lax.rsqrt(total / full + EPSILON)

    def own_copy(d, c):
        return pltpu.make_async_remote_copy(
            x_ref.at[:, col(c)], xs.at[z, :, col(c)], own_sem.at[d, c], blk_sem.at[z, c],
            device_id=outward if d else inward,
        )

    def relay(s, c):
        b = block(s)
        return pltpu.make_async_remote_copy(
            xs.at[b, :, col(c)], xs.at[b, :, col(c)], rel_sem.at[s - 1, c], blk_sem.at[b, c],
            device_id=inward if s == 1 else outward,
        )

    def own_note(d):
        return pltpu.make_async_remote_copy(
            note_s, notes.at[z], nown_sem.at[d], note_sem.at[z], device_id=outward if d else inward
        )

    def relay_note(s):
        b = block(s)
        return pltpu.make_async_remote_copy(
            notes.at[b], notes.at[b], nrel_sem.at[s - 1], note_sem.at[b],
            device_id=inward if s == 1 else outward,
        )

    def pack_copy(s, c):
        return pltpu.make_async_remote_copy(
            pk_s.at[s, pl.ds(count, count), col(c)], pk_r.at[s, :, col(c)], ks_sem.at[s, c], kr_sem.at[s, c],
            device_id=across,
        )

    def ret_copy(s, c, at):
        return pltpu.make_async_remote_copy(
            ret_s.at[s, :, at(c)], ret_r.at[s, :, at(c)], ts_sem.at[s, c], tr_sem.at[s, c],
            device_id=across,
        )

    def sum_copy(s, c, at):
        slot = jnp.where(end, spare, block(s)) if s == 1 else block(s)
        ep = jnp.where(inner, outward["ep"], inward["ep"]) if s == 1 else inward["ep"]
        return pltpu.make_async_remote_copy(
            sum_s.at[s - 1, :, at(c)], sum_r.at[slot, :, at(c)], ss_sem.at[s - 1, c], sr_sem.at[slot, c],
            device_id={"ep": ep, "tp": my_tp},
        )

    def sum_wait(slot, c, at):
        pltpu.make_async_remote_copy(
            sum_s.at[0, :, at(c)], sum_r.at[slot, :, at(c)], ss_sem.at[0, c], sr_sem.at[slot, c],
            device_id=inward,
        ).wait_recv()

    def p_copy(i, o):
        q = lax.rem(my_tp + o, nt)
        return pltpu.make_async_remote_copy(
            part.at[i, q], recv_p.at[i, o - 1], ps_sem.at[i, o - 1], pr_sem.at[i, o - 1],
            device_id={"ep": me, "tp": q},
        )

    def h_copy(i, o, back=False):
        mine = lax.rem(my_tp - o + nt, nt) if back else my_tp
        q = lax.rem(my_tp - o + nt, nt) if back else lax.rem(my_tp + o, nt)
        return pltpu.make_async_remote_copy(
            hid.at[i, mine], hid.at[i, mine], hs_sem.at[i, o - 1], hr_sem.at[i, o - 1],
            device_id={"ep": me, "tp": q},
        )

    def prepare(s):
        meta = notes[block(s)] if s else note_s[...]
        row = lax.broadcasted_iota(jnp.int32, (16, rows_all), 0)
        name = jnp.where(row < local, me * local + row, mate * local + row - local)
        name = jnp.where(row < 2 * local, name, -1).astype(F32)
        first, second = meta[0:1] == name, meta[1:2] == name
        hit = first | second
        before = dot(jnp.where(hit, 1.0, 0.0).astype(BF), tri[...])
        rank = jnp.where(hit, before, -1.0)
        weight = jnp.where(first, meta[2:3], 0.0) + jnp.where(second, meta[3:4], 0.0)
        blank = jnp.zeros((128 - 32, rows_all), F32)
        cols[s] = jnp.concatenate([rank, weight, blank], axis=0).T
        spot = lax.broadcasted_iota(jnp.int32, (cap, rows_all), 0).astype(F32)
        for e in range(2 * local):
            at = pl.ds(e * cap, cap)
            here = spot == rank[e:e + 1]
            pick[at, :] = jnp.where(here, 1.0, 0.0).astype(BF)
            total = jnp.sum(jnp.where(here, meta[4:5], 0.0), axis=1, keepdims=True)
            lift[at, :] = jnp.broadcast_to(total, (cap, lift.shape[1]))

    def pack(s, c):
        values = x_ref.at[:, col(c)] if s == 0 else xs.at[block(s), :, col(c)]

        @pl.loop(0, 2 * local)
        def _(e):
            group = pl.ds(pl.multiple_of(e * cap, cap), cap)
            rows = dot(pick[group, :], values[...]) * lift[group, 0:1] * gain_ref[:, col(c)]
            pk_s[s, group, col(c)] = rows.astype(BF)

        pack_copy(s, c).start()

    def stage_a(s, h):
        i = 2 * s + h
        if h:
            for c in range(parts):
                pack_copy(s, c).wait_recv()
        source = pk_r if h else pk_s

        @pl.loop(0, local)
        def _(j):
            group = pl.ds(pl.multiple_of(j * cap, cap), cap)
            rows = source[s, group, :]
            gate = dot(rows, gate_v[j]).astype(BF)
            upper = dot(rows, up_v[j]).astype(BF)
            for q in range(nt):
                part[i, q, group, pl.ds(0, fq)] = gate[:, q * fq:(q + 1) * fq]
                part[i, q, group, pl.ds(fq, fq)] = upper[:, q * fq:(q + 1) * fq]

        for o in range(1, nt):
            p_copy(i, o).start()

    def stage_b(s, h):
        i = 2 * s + h
        for o in range(1, nt):
            p_copy(i, o).wait_recv()
        total = part[i, my_tp].astype(F32)
        for o in range(1, nt):
            total = total + recv_p[i, o - 1].astype(F32)
        gate, upper = total[:, :fq], total[:, fq:]
        hid[i, my_tp] = (gate / (1.0 + jnp.exp(-gate)) * upper).astype(BF)
        for o in range(1, nt):
            h_copy(i, o).start()

    def hidden(s, h, j):
        return jnp.concatenate([hid[2 * s + h, q, pl.ds(j * cap, cap), :] for q in range(nt)], axis=1)

    def take_hidden(s, h):
        for o in range(1, nt):
            h_copy(2 * s + h, o, True).wait_recv()

    def stage_c(s):
        take_hidden(s, 0)
        for j in range(local):
            out_o[s, pl.ds(j * cap, cap), :] = dot(hidden(s, 0, j), down_v[j]).astype(BF)

    def send_back(s, c):
        if c == 0:
            take_hidden(s, 1)
        for j in range(local):
            ret_s[s, pl.ds(j * cap, cap), col(c)] = dot(hidden(s, 1, j), down_v[j, :, col(c)]).astype(BF)
        ret_copy(s, c, col).start()

    def weave(s):
        table = cols[s]
        spot = lax.broadcasted_iota(jnp.int32, (rows_all, cap), 1).astype(F32)
        for e in range(2 * local):
            here = spot == table[:, e:e + 1]
            comb[s, :, pl.ds(e * cap, cap)] = jnp.where(here, table[:, 16 + e:17 + e], 0.0).astype(BF)

    def mix(s, c, put):
        ret_copy(s, c, col).wait_recv()

        @pl.loop(0, 2)
        def _(k):
            group = pl.ds(pl.multiple_of(k * (rows_all // 2), rows_all // 2), rows_all // 2)
            near = dot(comb[s, group, pl.ds(0, count)], out_o[s, :, col(c)])
            put(group, near + dot(comb[s, group, pl.ds(count, count)], ret_r[s, :, col(c)]))

    def stage_d(s, c, more):
        if more:
            sum_wait(block(s), c, col)

        def put(group, total):
            if more:
                total = total + sum_r[block(s), group, col(c)].astype(F32)
            sum_s[s - 1, group, col(c)] = total.astype(BF)

        mix(s, c, put)
        sum_copy(s, c, col).start()

    def own_mix(c):
        def put(group, total):
            acc[group, col(c)] = total

        mix(0, c, put)

    def add_spare(c):
        sum_wait(spare, c, col)
        acc[:, col(c)] += sum_r[spare, :, col(c)].astype(F32)

    def add_last(c):
        sum_wait(z, c, col)
        acc[:, col(c)] += sum_r[z, :, col(c)].astype(F32)

    def pass_on(s, c):
        relay(s, c).wait_recv()
        relay(s, c).start()

    def pass_note(s):
        relay_note(s).wait_recv()
        relay_note(s).start()

    def arrive(s, c):
        relay(s, c).wait_recv()

    def take_note(s):
        relay_note(s).wait_recv()

    def lead(k):
        own_copy(0, k).start()

    def run(order, at_end):
        def prep(s):
            if at_end:
                take_note(s)
            prepare(s)

        def bring(s, c):
            if at_end:
                arrive(s, c)
            pack(s, c)

        calls = {
            "passn": pass_note, "pass": pass_on, "ownin": lead, "prep": prep, "pack": bring,
            "a": stage_a, "b": stage_b, "c": stage_c, "c1": send_back, "weave": weave, "mix0": own_mix,
            "d": lambda s, c: stage_d(s, c, not at_end), "spare": add_spare, "last": add_last,
        }
        for name, *where in order:
            calls[name](*where)

    pl.semaphore_wait(barrier, jnp.where(inner, 3, 2) + nt - 1)
    x_loads[0].wait()
    own_copy(0, 0).start()

    @pl.when(inner)
    def _():
        own_copy(1, 0).start()

    for load in x_loads[1:]:
        load.wait()
    values = x_ref[...].astype(F32)
    start_sum(0, jnp.sum(values * values, axis=1, keepdims=True))
    send_sum(0)
    shape = (rows_all, rows_all)
    earlier = lax.broadcasted_iota(jnp.int32, shape, 0) < lax.broadcasted_iota(jnp.int32, shape, 1)
    tri[...] = jnp.where(earlier, 1.0, 0.0).astype(BF)
    blank = jnp.zeros((3, rows_all), F32)
    note_s[...] = jnp.concatenate(
        [route_ref[...].astype(F32), weight_ref[...], finish_sum(0)[0:1], blank], axis=0
    )
    own_note(0).start()

    @pl.when(inner)
    def _():
        own_note(1).start()
        for c in range(1, parts // 2):
            own_copy(0, c).start()
        for c in range(1, parts):
            own_copy(1, c).start()

    @pl.when(end)
    def _():
        for c in range(1, parts):
            own_copy(0, c).start()

    prepare(0)
    for c in range(parts):
        pack(0, c)
    for load in loads:
        load.wait()

    @pl.when(end)
    def _():
        run(END_ORDER, True)

    @pl.when(inner)
    def _():
        run(INNER_ORDER, False)

    summed = acc[...]
    start_sum(1, jnp.sum(summed * summed, axis=1, keepdims=True))
    send_sum(1)

    for i in range(2 * last + 2):
        for o in range(1, nt):
            p_copy(i, o).wait_send()
            h_copy(i, o).wait_send()
    for s in range(last + 1):
        for c in range(parts):
            pack_copy(s, c).wait_send()
            ret_copy(s, c, col).wait_send()
            if s:
                sum_copy(s, c, col).wait_send()
    for c in range(parts):
        own_copy(0, c).wait_send()
    own_note(0).wait_send()

    @pl.when(inner)
    def _():
        own_note(1).wait_send()
        for c in range(parts):
            own_copy(1, c).wait_send()
        for s in range(1, last + 1):
            relay_note(s).wait_send()
            for c in range(parts):
                relay(s, c).wait_send()

    scale = jnp.sum(jnp.where(eye(), finish_sum(1)[0:1], 0.0), axis=1, keepdims=True)
    out_ref[...] = (acc[...] * scale * last_gain_ref[...]).astype(BF)
    for k in range(2):
        for o in range(1, nt):
            sq_copy(k, o).wait_send()


def line_call(n, nt, local, cap, full, tokens, routes, weights, norm_gain, gate_weight, up_weight, down_weight, final_gain):
    rows, width = tokens.shape
    ff = gate_weight.shape[2]
    line = n // 2
    count = local * cap
    parts = 4
    any_spec = pl.BlockSpec(memory_space=pl.ANY)
    vmem = pl.BlockSpec(memory_space=pltpu.VMEM)
    dma = pltpu.SemaphoreType.DMA
    return pl.pallas_call(
        functools.partial(line_kernel, n, nt, local, cap, full, parts),
        out_shape=jax.ShapeDtypeStruct((rows, width), BF),
        in_specs=[any_spec, vmem, vmem, vmem, vmem, any_spec, any_spec, any_spec],
        out_specs=vmem,
        scratch_shapes=[
            pltpu.VMEM(gate_weight.shape, BF),
            pltpu.VMEM(up_weight.shape, BF),
            pltpu.VMEM(down_weight.shape, BF),
            pltpu.VMEM((rows, width), BF),
            pltpu.VMEM((line, rows, width), BF),
            pltpu.VMEM((line, 8, rows), F32),
            pltpu.VMEM((8, rows), F32),
            pltpu.VMEM((rows, rows), BF),
            pltpu.VMEM((line, rows, 128), F32),
            pltpu.VMEM((2 * count, rows), BF),
            pltpu.VMEM((2 * count, 128), F32),
            pltpu.VMEM((line, 2 * count, width), BF),
            pltpu.VMEM((line, count, width), BF),
            pltpu.VMEM((n, nt, count, 2 * ff // nt), BF),
            pltpu.VMEM((n, nt - 1, count, 2 * ff // nt), BF),
            pltpu.VMEM((n, nt, count, ff // nt), BF),
            pltpu.VMEM((line, count, width), BF),
            pltpu.VMEM((line, count, width), BF),
            pltpu.VMEM((line, count, width), BF),
            pltpu.VMEM((line, rows, 2 * count), BF),
            pltpu.VMEM((line - 1, rows, width), BF),
            pltpu.VMEM((line + 1, rows, width), BF),
            pltpu.VMEM((rows, width), F32),
            pltpu.VMEM((2, 8, rows), F32),
            pltpu.VMEM((2, nt - 1, 8, rows), F32),
            dma((3,)),
            dma((parts,)),
            dma((2, parts)),
            dma((line - 1, parts)),
            dma((line, parts)),
            dma((2,)),
            dma((line - 1,)),
            dma((line,)),
            dma((line, parts)),
            dma((line, parts)),
            dma((n, nt - 1)),
            dma((n, nt - 1)),
            dma((n, nt - 1)),
            dma((n, nt - 1)),
            dma((line, parts)),
            dma((line, parts)),
            dma((line - 1, parts)),
            dma((line + 1, parts)),
            dma((2, nt - 1)),
            dma((2, nt - 1)),
        ],
        compiler_params=pltpu.CompilerParams(
            collective_id=0, has_side_effects=True, vmem_limit_bytes=62 * 1024 * 1024
        ),
    )(tokens, routes.T, weights.T, norm_gain[None], final_gain[None], gate_weight, up_weight, down_weight)


RING_BYTES = 24 * 1024 * 1024


def body(tokens, routes, route_weights, norm_gain, gate_weight, up_weight, down_weight, final_gain):
    n, nt = lax.axis_size("ep"), lax.axis_size("tp")
    local, width, ff = gate_weight.shape
    experts = n * local
    rows = tokens.shape[0]
    full = width * nt
    cap = 4 * rows // experts
    count = local * cap
    blocks = max(n - 4, 0)
    ring = n % 2 == 0 and n >= 6 and local % 2 == 0 and blocks * rows * width * 2 <= RING_BYTES
    if n == 8 and local <= 8 and width % 512 == 0 and cap % 128 == 0:
        return line_call(
            n, nt, local, cap, full, tokens, routes, route_weights, norm_gain, gate_weight, up_weight, down_weight, final_gain
        )
    meta = jnp.concatenate(
        [routes.T.astype(F32), route_weights.T, jnp.zeros((4, rows), F32)], axis=0
    )
    tables = 1 + blocks if ring else 1
    packed = count + local // 2 * cap

    any_spec = pl.BlockSpec(memory_space=pl.ANY)
    vmem = pl.BlockSpec(memory_space=pltpu.VMEM)
    dma = pltpu.SemaphoreType.DMA

    def only(ring_shape, shape, kind=BF):
        return pltpu.VMEM(ring_shape if ring else shape, kind)

    tiny = (1, 16, 128)
    return pl.pallas_call(
        functools.partial(kernel, n, nt, local, cap, ring, full),
        out_shape=jax.ShapeDtypeStruct((rows, width), BF),
        in_specs=[vmem, vmem, vmem, vmem, any_spec, any_spec, any_spec],
        out_specs=vmem,
        scratch_shapes=[
            pltpu.VMEM(gate_weight.shape, BF),
            pltpu.VMEM(up_weight.shape, BF),
            pltpu.VMEM(down_weight.shape, BF),
            pltpu.VMEM((rows, width), BF),
            pltpu.VMEM((rows, width), F32),
            pltpu.VMEM((rows, rows), BF),
            pltpu.VMEM((tables, experts, rows), F32),
            pltpu.VMEM((tables, experts, rows), F32),
            pltpu.VMEM((2, 8, rows), F32),
            pltpu.VMEM((2, nt - 1, 8, rows), F32),
            only(tiny, (n, count, width)),
            only((blocks, rows, width), (n, count, width)),
            only((2, packed, width), tiny),
            only((2, packed, width), tiny),
            only((2, local // 2 * cap, width), tiny),
            only((blocks, 8, rows), (1, 8, 128), F32),
            pltpu.VMEM((n, nt, count, 2 * ff // nt), BF),
            pltpu.VMEM((n, nt - 1, count, 2 * ff // nt), BF),
            pltpu.VMEM((n, nt, count, ff // nt), BF),
            pltpu.VMEM((n, count, width), BF),
            pltpu.VMEM((n, count, width), BF),
            dma((3,)),
            dma((blocks, 2) if ring else (n,)),
            dma((blocks, 2) if ring else (n,)),
            dma((2,)),
            dma((2,)),
            dma((2,)),
            dma((2,)),
            dma((blocks,) if ring else (1,)),
            dma((blocks,) if ring else (1,)),
            dma((n, nt - 1)),
            dma((n, nt - 1)),
            dma((n, nt - 1)),
            dma((n, nt - 1)),
            dma((n,)),
            dma((n,)),
            dma((2, nt - 1)),
            dma((2, nt - 1)),
        ],
        compiler_params=pltpu.CompilerParams(
            collective_id=0, has_side_effects=True, vmem_limit_bytes=60 * 1024 * 1024
        ),
    )(tokens, meta, norm_gain[None], final_gain[None], gate_weight, up_weight, down_weight)


def solution(mesh):
    in_specs = (
        P("ep", "tp"),
        P("ep", None),
        P("ep", None),
        P("tp"),
        P("ep", "tp", None),
        P("ep", "tp", None),
        P("ep", None, "tp"),
        P("tp"),
    )
    return jax.shard_map(body, mesh=mesh, in_specs=in_specs, out_specs=P("ep", "tp"), check_vma=False)
```

```python
import functools

import jax
import jax.numpy as jnp
from jax import lax
from jax.experimental import pallas as pl
from jax.experimental.pallas import tpu as pltpu
from jax.sharding import PartitionSpec as P

EPSILON = 1e-06
BF = jnp.bfloat16
F32 = jnp.float32


def dot(a, b):
    return jnp.dot(a, b, preferred_element_type=F32)


def dot_t(a, b):
    return lax.dot_general(a, b, (((0,), (0,)), ((), ())), preferred_element_type=F32)


def kernel(
    n, nt, local, cap, ring, full,
    x_ref, meta_ref, gain_ref, last_gain_ref, gate_hbm, up_hbm, down_hbm, out_ref,
    gate_v, up_v, down_v, xn, acc, tri, rank_t, wt_t, sq, sq2,
    send_x, recv_x, pk_s, pk_r, far_r, meta_r,
    part, recv_p, hid, out_s, out_r,
    w_sem, xs_sem, xr_sem, ks_sem, kr_sem, fs_sem, fr_sem, ms_sem, mr_sem,
    ps_sem, pr_sem, hs_sem, hr_sem, os_sem, or_sem, qs_sem, qr_sem,
):
    me = lax.axis_index("ep")
    my_tp = lax.axis_index("tp")
    ff = gate_v.shape[2]
    fq = ff // nt
    rows_all = x_ref.shape[0]
    half = n // 2
    chunk = rows_all // 2
    count = local * cap
    split = local // 2

    loads = [
        pltpu.make_async_copy(src, dst, w_sem.at[i])
        for i, (src, dst) in enumerate(((gate_hbm, gate_v), (up_hbm, up_v), (down_hbm, down_v)))
    ]
    for load in loads:
        load.start()

    barrier = pltpu.get_barrier_semaphore()

    @pl.loop(1, n)
    def _(s):
        pl.semaphore_signal(barrier, inc=1, device_id={"ep": lax.rem(me + s, n), "tp": my_tp})

    for o in range(1, nt):
        pl.semaphore_signal(barrier, inc=1, device_id={"ep": me, "tp": lax.rem(my_tp + o, nt)})

    place = jnp.where(me % 2 == 0, me // 2, n - 1 - me // 2)

    def at_place(p):
        p = lax.rem(p + 2 * n, n)
        return jnp.where(p < half, 2 * p, 2 * (n - 1 - p) + 1)

    def shift(s):
        return (1 - 2 * ((s + 1) % 2)) * ((s + 1) // 2)

    def source(s):
        if ring:
            return at_place(place - shift(s))
        return lax.rem(me - s + n, n)

    def sender(s):
        if ring:
            return at_place(place + shift(s))
        return lax.rem(me + s, n)

    def eye():
        shape = (rows_all, rows_all)
        return lax.broadcasted_iota(jnp.int32, shape, 0) == lax.broadcasted_iota(jnp.int32, shape, 1)

    def sq_copy(k, o):
        q = lax.rem(my_tp + o, nt)
        return pltpu.make_async_remote_copy(
            sq.at[k], sq2.at[k, o - 1], qs_sem.at[k, o - 1], qr_sem.at[k, o - 1],
            device_id={"ep": me, "tp": q},
        )

    def start_sum(k, column):
        row = jnp.sum(jnp.where(eye(), column, 0.0), axis=0, keepdims=True)
        sq[k] = jnp.broadcast_to(row, sq.shape[1:])

    def send_sum(k):
        for o in range(1, nt):
            sq_copy(k, o).start()

    def finish_sum(k):
        for o in range(1, nt):
            sq_copy(k, o).wait_recv()
        total = sq[k]
        for o in range(1, nt):
            total = total + sq2[k, o - 1]
        scale = lax.rsqrt(total[0:1] / full + EPSILON)
        return jnp.sum(jnp.where(eye(), scale, 0.0), axis=1, keepdims=True)

    def make_table(slot, meta):
        names = lax.broadcasted_iota(jnp.int32, rank_t.shape[1:], 0).astype(F32)
        first, second = meta[0:1] == names, meta[1:2] == names
        hit = first | second
        before = dot(jnp.where(hit, 1.0, 0.0).astype(BF), tri[...])
        rank_t[slot] = jnp.where(hit, before, -1.0)
        wt_t[slot] = jnp.where(first, meta[2:3], 0.0) + jnp.where(second, meta[3:4], 0.0)

    def onehot(slot, expert, weighted=False):
        rank = rank_t[slot, pl.ds(expert, 1), :]
        hit = lax.broadcasted_iota(jnp.int32, (cap, rows_all), 0).astype(F32) == rank
        return jnp.where(hit, wt_t[slot, pl.ds(expert, 1), :] if weighted else F32(1.0), F32(0.0))

    def pack(slot, experts, block):
        pick = jnp.concatenate([onehot(slot, e) for e in experts], axis=0).astype(BF)
        return dot(pick, block).astype(BF)

    def experts_of(owner):
        return [owner * local + j for j in range(local)]

    def x_copy(s):
        return pltpu.make_async_remote_copy(
            send_x.at[s], recv_x.at[s], xs_sem.at[s], xr_sem.at[s],
            device_id={"ep": sender(s), "tp": my_tp},
        )

    def ahead(i):
        return {"ep": at_place(place + 1 - 2 * i), "tp": my_tp}

    def block_copy(d, i, k):
        piece = pl.ds(k * chunk, chunk)
        src = xn.at[piece] if d == 1 else recv_x.at[2 * d - 4 + i, piece]
        slot = 2 * d - 2 + i
        return pltpu.make_async_remote_copy(
            src, recv_x.at[slot, piece], xs_sem.at[slot, k], xr_sem.at[slot, k], device_id=ahead(i)
        )

    def meta_copy(d, i):
        slot = 2 * d - 2 + i
        return pltpu.make_async_remote_copy(
            meta_ref if d == 1 else meta_r.at[slot - 2], meta_r.at[slot],
            ms_sem.at[slot], mr_sem.at[slot], device_id=ahead(i),
        )

    def pack_copy(i):
        return pltpu.make_async_remote_copy(
            pk_s.at[i], pk_r.at[i], ks_sem.at[i], kr_sem.at[i], device_id=ahead(i)
        )

    def far_copy(i):
        return pltpu.make_async_remote_copy(
            pk_r.at[i, pl.ds(count, split * cap)], far_r.at[i], fs_sem.at[i], fr_sem.at[i],
            device_id=ahead(i),
        )

    def p_copy(s, o):
        q = lax.rem(my_tp + o, nt)
        return pltpu.make_async_remote_copy(
            part.at[s, q], recv_p.at[s, o - 1], ps_sem.at[s, o - 1], pr_sem.at[s, o - 1],
            device_id={"ep": me, "tp": q},
        )

    def h_copy(s, o, back=False):
        mine = lax.rem(my_tp - o + nt, nt) if back else my_tp
        q = lax.rem(my_tp - o + nt, nt) if back else lax.rem(my_tp + o, nt)
        return pltpu.make_async_remote_copy(
            hid.at[s, mine], hid.at[s, mine], hs_sem.at[s, o - 1], hr_sem.at[s, o - 1],
            device_id={"ep": me, "tp": q},
        )

    def o_copy(s):
        return pltpu.make_async_remote_copy(
            out_s.at[s], out_r.at[s], os_sem.at[s], or_sem.at[s],
            device_id={"ep": source(s), "tp": my_tp},
        )

    def stage_a(s, rows_of):
        for j in range(local):
            rows = rows_of(j)
            gate = dot(rows, gate_v[j]).astype(BF)
            upper = dot(rows, up_v[j]).astype(BF)
            for q in range(nt):
                part[s, q, pl.ds(j * cap, cap), pl.ds(0, fq)] = gate[:, q * fq:(q + 1) * fq]
                part[s, q, pl.ds(j * cap, cap), pl.ds(fq, fq)] = upper[:, q * fq:(q + 1) * fq]
        for o in range(1, nt):
            p_copy(s, o).start()

    def stage_b(s):
        for o in range(1, nt):
            p_copy(s, o).wait_recv()
        total = part[s, my_tp].astype(F32)
        for o in range(1, nt):
            total = total + recv_p[s, o - 1].astype(F32)
        gate, upper = total[:, :fq], total[:, fq:]
        hid[s, my_tp] = (gate / (1.0 + jnp.exp(-gate)) * upper).astype(BF)
        for o in range(1, nt):
            h_copy(s, o).start()

    def stage_c(s, own):
        for o in range(1, nt):
            h_copy(s, o, True).wait_recv()
        target = out_r if own else out_s
        for j in range(local):
            hidden = jnp.concatenate([hid[s, q, pl.ds(j * cap, cap), :] for q in range(nt)], axis=1)
            target[s, pl.ds(j * cap, cap), :] = dot(hidden, down_v[j]).astype(BF)
        if not own:
            o_copy(s).start()

    def combine(s):
        weight = jnp.concatenate([onehot(0, e, True) for e in experts_of(sender(s))], axis=0)
        high = weight.astype(BF)
        low = (weight - high.astype(F32)).astype(BF)
        rows = out_r[s]
        return dot_t(high, rows) + dot_t(low, rows)

    values = x_ref[...].astype(F32)
    start_sum(0, jnp.sum(values * values, axis=1, keepdims=True))
    shape = (rows_all, rows_all)
    earlier = lax.broadcasted_iota(jnp.int32, shape, 0) < lax.broadcasted_iota(jnp.int32, shape, 1)
    tri[...] = jnp.where(earlier, 1.0, 0.0).astype(BF)
    pl.semaphore_wait(barrier, n - 1 + nt - 1)
    send_sum(0)
    if ring:
        for i in range(2):
            meta_copy(1, i).start()
    make_table(0, meta_ref[...])
    scale = finish_sum(0)
    xn[...] = (x_ref[...].astype(F32) * scale * gain_ref[...]).astype(BF)

    def own_rows(j):
        return pack(0, [me * local + j], xn[...])

    def stored(ref, slot):
        return lambda j: ref[slot, pl.ds(j * cap, cap), :]

    if ring:
        for k in range(2):
            for i in range(2):
                block_copy(1, i, k).start()
        for load in loads:
            load.wait()
        stage_a(0, own_rows)
        for d in range(1, half + 1):
            if d <= half - 2:
                for k in range(2):
                    for i in range(2):
                        block_copy(d, i, k).wait_recv()
                        if d < half - 2:
                            block_copy(d + 1, i, k).start()
                for i in range(2):
                    slot = 2 * d - 2 + i
                    meta_copy(d, i).wait_recv()
                    if d < half - 2:
                        meta_copy(d + 1, i).start()
                    make_table(1 + slot, meta_r[slot])
                if d == half - 2:
                    for i in range(2):
                        slot = 2 * d - 2 + i
                        step = 1 - 2 * i
                        far = experts_of(at_place(place + 2 * step))
                        wanted = experts_of(at_place(place + step)) + (far[split:] if i else far[:split])
                        pk_s[i] = pack(1 + slot, wanted, recv_x[slot])
                        pack_copy(i).start()
            elif d == half - 1:
                for i in range(2):
                    pack_copy(i).wait_recv()
                    far_copy(i).start()
            else:
                for i in range(2):
                    far_copy(i).wait_recv()
            for i in range(2 if d < half else 1):
                s = 2 * d - 1 + i
                slot = s - 1
                if d <= half - 2:
                    stage_a(s, lambda j, slot=slot: pack(1 + slot, [me * local + j], recv_x[slot]))
                elif d == half - 1:
                    stage_a(s, stored(pk_r, i))
                else:
                    stage_a(s, lambda j: far_r[j // split, pl.ds(j % split * cap, cap), :])
                stage_b(s - 1)
                if s >= 2:
                    stage_c(s - 2, s == 2)
    else:
        send_x[1] = pack(0, experts_of(sender(1)), xn[...])

        @pl.loop(2, n)
        def _(s):
            send_x[s] = pack(0, experts_of(sender(s)), xn[...])
            x_copy(s - 1).start()

        for load in loads:
            load.wait()
        stage_a(0, own_rows)
        x_copy(n - 1).start()
        x_copy(1).wait_recv()
        stage_a(1, stored(recv_x, 1))
        stage_b(0)
        x_copy(2).wait_recv()
        stage_a(2, stored(recv_x, 2))
        stage_b(1)
        stage_c(0, True)

        @pl.loop(3, n)
        def _(s):
            x_copy(s).wait_recv()
            stage_a(s, stored(recv_x, s))
            stage_b(s - 1)
            stage_c(s - 2, False)

    stage_b(n - 1)
    stage_c(n - 2, False)
    acc[...] = combine(0)
    stage_c(n - 1, False)

    @pl.loop(1, n)
    def _(s):
        o_copy(s).wait_recv()
        acc[...] += combine(s)

    summed = acc[...]
    start_sum(1, jnp.sum(summed * summed, axis=1, keepdims=True))

    @pl.loop(0, n)
    def _(s):
        for o in range(1, nt):
            p_copy(s, o).wait_send()
            h_copy(s, o).wait_send()

    send_sum(1)

    @pl.loop(1, n)
    def _(s):
        o_copy(s).wait_send()

    if ring:
        for i in range(2):
            for d in range(1, half - 1):
                meta_copy(d, i).wait_send()
                for k in range(2):
                    block_copy(d, i, k).wait_send()
            pack_copy(i).wait_send()
            far_copy(i).wait_send()
    else:
        @pl.loop(1, n)
        def _(s):
            x_copy(s).wait_send()

    scale = finish_sum(1)
    out_ref[...] = (acc[...] * scale * last_gain_ref[...]).astype(BF)
    for k in range(2):
        for o in range(1, nt):
            sq_copy(k, o).wait_send()


END_ORDER = (
    ("prep", 1), ("a", 0, 0), ("pack", 1, 0), ("b", 0, 0), ("pack", 1, 1), ("pack", 1, 2), ("a", 0, 1), ("b",
    0, 1), ("pack", 1, 3), ("prep", 2), ("a", 1, 0), ("a", 1, 1), ("c1", 0, 0), ("weave", 1), ("pack", 2, 0),
    ("pack", 2, 1), ("b", 1, 0), ("b", 1, 1), ("pack", 2, 2), ("pack", 2, 3), ("a", 2, 0), ("c1", 1, 0),
    ("c1", 1, 1), ("c1", 1, 2), ("a", 2, 1), ("c", 1), ("d", 1, 0), ("b", 2, 0), ("prep", 3), ("pack", 3, 0),
    ("pack", 3, 1), ("weave", 2), ("d", 1, 1), ("b", 2, 1), ("d", 1, 2), ("pack", 3, 2), ("c1", 2, 0),
    ("pack", 3, 3), ("c1", 2, 1), ("a", 3, 0), ("c", 2), ("d", 2, 0), ("c1", 2, 2), ("c1", 2, 3), ("c1", 0,
    1), ("a", 3, 1), ("d", 2, 1), ("d", 2, 3), ("b", 3, 1), ("b", 3, 0), ("weave", 0), ("d", 2, 2), ("c1", 1,
    3), ("weave", 3), ("c", 0), ("c1", 3, 0), ("c1", 3, 1), ("c", 3), ("d", 3, 0), ("mix0", 1), ("c1", 0, 2),
    ("d", 3, 1), ("c1", 3, 2), ("c1", 3, 3), ("d", 3, 2), ("mix0", 0), ("c1", 0, 3), ("d", 3, 3), ("mix0", 2),
    ("last", 0), ("mix0", 3), ("last", 3), ("d", 1, 3), ("last", 1), ("last", 2),
)

INNER_ORDER = (
    ("a", 0, 0), ("passn", 1), ("prep", 1), ("pass", 1, 0), ("b", 0, 0), ("pass", 1, 1), ("pack", 1, 0),
    ("pack", 1, 1), ("a", 0, 1), ("weave", 0), ("passn", 2), ("pass", 2, 0), ("pass", 1, 2), ("pack", 1, 2),
    ("pass", 1, 3), ("c", 0), ("pack", 1, 3), ("prep", 2), ("pass", 2, 1), ("pass", 2, 2), ("a", 1, 0),
    ("pass", 2, 3), ("ownin", 2), ("ownin", 3), ("pack", 2, 0), ("b", 0, 1), ("pack", 2, 1), ("pack", 2, 2),
    ("a", 1, 1), ("pack", 2, 3), ("passn", 3), ("weave", 1), ("c1", 0, 0), ("prep", 3), ("pass", 3, 0), ("a",
    2, 0), ("pass", 3, 1), ("pack", 3, 0), ("b", 1, 0), ("pass", 3, 2), ("pass", 3, 3), ("a", 2, 1), ("pack",
    3, 1), ("pack", 3, 2), ("b", 1, 1), ("b", 2, 1), ("pack", 3, 3), ("a", 3, 0), ("c1", 0, 1), ("mix0", 1),
    ("mix0", 0), ("c1", 2, 0), ("b", 2, 0), ("c1", 2, 1), ("c1", 2, 2), ("c1", 2, 3), ("weave", 2), ("b", 3,
    0), ("weave", 3), ("a", 3, 1), ("c1", 1, 0), ("c", 2), ("d", 2, 0), ("b", 3, 1), ("d", 2, 1), ("c1", 1,
    1), ("c1", 1, 2), ("c1", 1, 3), ("c", 3), ("c", 1), ("d", 1, 0), ("c1", 3, 0), ("d", 2, 3), ("d", 1, 1),
    ("d", 2, 2), ("c1", 3, 1), ("c1", 3, 2), ("c1", 3, 3), ("c1", 0, 2), ("c1", 0, 3), ("d", 1, 3), ("d", 3,
    0), ("d", 1, 2), ("d", 3, 1), ("d", 3, 2), ("mix0", 3), ("spare", 1), ("d", 3, 3), ("last", 1), ("spare",
    0), ("last", 0), ("mix0", 2), ("spare", 2), ("spare", 3), ("last", 2), ("last", 3),
)


def line_kernel(
    n, nt, local, cap, full, parts,
    x_hbm, route_hbm, weight_hbm, gain_hbm, last_gain_hbm, gate_hbm, up_hbm, down_hbm, out_ref,
    gate_v, up_v, down_v, route_ref, weight_ref, gain_ref, last_gain_ref, x_ref, xs, notes, note_s, tri, cols, pick, lift, pk_s, pk_r,
    part, recv_p, hid, out_o, ret_s, ret_r, comb, sum_s, sum_r, acc, sq, sq2,
    w_sem, small_sem, x_sem, own_sem, rel_sem, blk_sem, nown_sem, nrel_sem, note_sem, ks_sem, kr_sem,
    ps_sem, pr_sem, hs_sem, hr_sem, ts_sem, tr_sem, ss_sem, sr_sem, qs_sem, qr_sem,
):
    me = lax.axis_index("ep")
    my_tp = lax.axis_index("tp")
    ff = gate_v.shape[2]
    fq = ff // nt
    rows_all, width = x_ref.shape
    cw = width // parts
    count = local * cap
    last = n // 2 - 1
    z, side = me // 2, me % 2
    low = z <= last // 2
    inner = (z >= 1) & (z <= last - 1)
    end = jnp.logical_not(inner)
    step_in = jnp.where(low, 2, -2)
    inward = {"ep": me + step_in, "tp": my_tp}
    outward = {"ep": jnp.where(inner, me - step_in, me + step_in), "tp": my_tp}
    mate = me + 1 - 2 * side
    across = {"ep": mate, "tp": my_tp}
    spare = last + 1

    def block(s):
        if s == 0:
            return z
        near = jnp.where(inner, 0, 1) if s == 1 else (last if s == 2 else last - 1)
        return jnp.where(low, near, last - near)

    loads = [
        pltpu.make_async_copy(src, dst, w_sem.at[i])
        for i, (src, dst) in enumerate(((gate_hbm, gate_v), (up_hbm, up_v), (down_hbm, down_v)))
    ]
    x_loads = [
        pltpu.make_async_copy(x_hbm.at[:, pl.ds(c * cw, cw)], x_ref.at[:, pl.ds(c * cw, cw)], x_sem.at[c])
        for c in range(parts)
    ]
    small = ((route_hbm, route_ref), (weight_hbm, weight_ref), (gain_hbm, gain_ref), (last_gain_hbm, last_gain_ref))
    small_loads = [pltpu.make_async_copy(src, dst, small_sem.at[i]) for i, (src, dst) in enumerate(small)]
    for load in x_loads + small_loads + loads:
        load.start()

    barrier = pltpu.get_barrier_semaphore()
    pl.semaphore_signal(barrier, inc=1, device_id=inward)
    pl.semaphore_signal(barrier, inc=1, device_id=across)

    @pl.when(inner)
    def _():
        pl.semaphore_signal(barrier, inc=1, device_id=outward)

    for o in range(1, nt):
        pl.semaphore_signal(barrier, inc=1, device_id={"ep": me, "tp": lax.rem(my_tp + o, nt)})

    def col(c):
        return pl.ds(c * cw, cw)

    def dcol(c):
        return pl.ds(pl.multiple_of(c * cw, cw), cw)

    def eye():
        shape = (rows_all, rows_all)
        return lax.broadcasted_iota(jnp.int32, shape, 0) == lax.broadcasted_iota(jnp.int32, shape, 1)

    def sq_copy(k, o):
        q = lax.rem(my_tp + o, nt)
        return pltpu.make_async_remote_copy(
            sq.at[k], sq2.at[k, o - 1], qs_sem.at[k, o - 1], qr_sem.at[k, o - 1],
            device_id={"ep": me, "tp": q},
        )

    def start_sum(k, column):
        row = jnp.sum(jnp.where(eye(), column, 0.0), axis=0, keepdims=True)
        sq[k] = jnp.broadcast_to(row, sq.shape[1:])

    def send_sum(k):
        for o in range(1, nt):
            sq_copy(k, o).start()

    def finish_sum(k):
        for o in range(1, nt):
            sq_copy(k, o).wait_recv()
        total = sq[k]
        for o in range(1, nt):
            total = total + sq2[k, o - 1]
        return lax.rsqrt(total / full + EPSILON)

    def own_copy(d, c):
        return pltpu.make_async_remote_copy(
            x_ref.at[:, col(c)], xs.at[z, :, col(c)], own_sem.at[d, c], blk_sem.at[z, c],
            device_id=outward if d else inward,
        )

    def relay(s, c):
        b = block(s)
        return pltpu.make_async_remote_copy(
            xs.at[b, :, col(c)], xs.at[b, :, col(c)], rel_sem.at[s - 1, c], blk_sem.at[b, c],
            device_id=inward if s == 1 else outward,
        )

    def own_note(d):
        return pltpu.make_async_remote_copy(
            note_s, notes.at[z], nown_sem.at[d], note_sem.at[z], device_id=outward if d else inward
        )

    def relay_note(s):
        b = block(s)
        return pltpu.make_async_remote_copy(
            notes.at[b], notes.at[b], nrel_sem.at[s - 1], note_sem.at[b],
            device_id=inward if s == 1 else outward,
        )

    def pack_copy(s, c):
        return pltpu.make_async_remote_copy(
            pk_s.at[s, pl.ds(count, count), col(c)], pk_r.at[s, :, col(c)], ks_sem.at[s, c], kr_sem.at[s, c],
            device_id=across,
        )

    def ret_copy(s, c, at):
        return pltpu.make_async_remote_copy(
            ret_s.at[s, :, at(c)], ret_r.at[s, :, at(c)], ts_sem.at[s, c], tr_sem.at[s, c],
            device_id=across,
        )

    def sum_copy(s, c, at):
        slot = jnp.where(end, spare, block(s)) if s == 1 else block(s)
        ep = jnp.where(inner, outward["ep"], inward["ep"]) if s == 1 else inward["ep"]
        return pltpu.make_async_remote_copy(
            sum_s.at[s - 1, :, at(c)], sum_r.at[slot, :, at(c)], ss_sem.at[s - 1, c], sr_sem.at[slot, c],
            device_id={"ep": ep, "tp": my_tp},
        )

    def sum_wait(slot, c, at):
        pltpu.make_async_remote_copy(
            sum_s.at[0, :, at(c)], sum_r.at[slot, :, at(c)], ss_sem.at[0, c], sr_sem.at[slot, c],
            device_id=inward,
        ).wait_recv()

    def p_copy(i, o):
        q = lax.rem(my_tp + o, nt)
        return pltpu.make_async_remote_copy(
            part.at[i, q], recv_p.at[i, o - 1], ps_sem.at[i, o - 1], pr_sem.at[i, o - 1],
            device_id={"ep": me, "tp": q},
        )

    def h_copy(i, o, back=False):
        mine = lax.rem(my_tp - o + nt, nt) if back else my_tp
        q = lax.rem(my_tp - o + nt, nt) if back else lax.rem(my_tp + o, nt)
        return pltpu.make_async_remote_copy(
            hid.at[i, mine], hid.at[i, mine], hs_sem.at[i, o - 1], hr_sem.at[i, o - 1],
            device_id={"ep": me, "tp": q},
        )

    def prepare(s):
        meta = notes[block(s)] if s else note_s[...]
        row = lax.broadcasted_iota(jnp.int32, (16, rows_all), 0)
        name = jnp.where(row < local, me * local + row, mate * local + row - local)
        name = jnp.where(row < 2 * local, name, -1).astype(F32)
        first, second = meta[0:1] == name, meta[1:2] == name
        hit = first | second
        before = dot(jnp.where(hit, 1.0, 0.0).astype(BF), tri[...])
        rank = jnp.where(hit, before, -1.0)
        weight = jnp.where(first, meta[2:3], 0.0) + jnp.where(second, meta[3:4], 0.0)
        blank = jnp.zeros((128 - 32, rows_all), F32)
        cols[s] = jnp.concatenate([rank, weight, blank], axis=0).T
        spot = lax.broadcasted_iota(jnp.int32, (cap, rows_all), 0).astype(F32)
        for e in range(2 * local):
            at = pl.ds(e * cap, cap)
            here = spot == rank[e:e + 1]
            pick[at, :] = jnp.where(here, 1.0, 0.0).astype(BF)
            total = jnp.sum(jnp.where(here, meta[4:5], 0.0), axis=1, keepdims=True)
            lift[at, :] = jnp.broadcast_to(total, (cap, lift.shape[1]))

    def pack(s, c):
        values = x_ref.at[:, col(c)] if s == 0 else xs.at[block(s), :, col(c)]

        @pl.loop(0, 2 * local)
        def _(e):
            group = pl.ds(pl.multiple_of(e * cap, cap), cap)
            rows = dot(pick[group, :], values[...]) * lift[group, 0:1] * gain_ref[:, col(c)]
            pk_s[s, group, col(c)] = rows.astype(BF)

        pack_copy(s, c).start()

    def stage_a(s, h):
        i = 2 * s + h
        if h:
            for c in range(parts):
                pack_copy(s, c).wait_recv()
        source = pk_r if h else pk_s

        @pl.loop(0, local)
        def _(j):
            group = pl.ds(pl.multiple_of(j * cap, cap), cap)
            rows = source[s, group, :]
            gate = dot(rows, gate_v[j]).astype(BF)
            upper = dot(rows, up_v[j]).astype(BF)
            for q in range(nt):
                part[i, q, group, pl.ds(0, fq)] = gate[:, q * fq:(q + 1) * fq]
                part[i, q, group, pl.ds(fq, fq)] = upper[:, q * fq:(q + 1) * fq]

        for o in range(1, nt):
            p_copy(i, o).start()

    def stage_b(s, h):
        i = 2 * s + h
        for o in range(1, nt):
            p_copy(i, o).wait_recv()
        total = part[i, my_tp].astype(F32)
        for o in range(1, nt):
            total = total + recv_p[i, o - 1].astype(F32)
        gate, upper = total[:, :fq], total[:, fq:]
        hid[i, my_tp] = (gate / (1.0 + jnp.exp(-gate)) * upper).astype(BF)
        for o in range(1, nt):
            h_copy(i, o).start()

    def hidden(s, h, j):
        return jnp.concatenate([hid[2 * s + h, q, pl.ds(j * cap, cap), :] for q in range(nt)], axis=1)

    def take_hidden(s, h):
        for o in range(1, nt):
            h_copy(2 * s + h, o, True).wait_recv()

    def stage_c(s):
        take_hidden(s, 0)
        for j in range(local):
            out_o[s, pl.ds(j * cap, cap), :] = dot(hidden(s, 0, j), down_v[j]).astype(BF)

    def send_back(s, c):
        if c == 0:
            take_hidden(s, 1)
        for j in range(local):
            ret_s[s, pl.ds(j * cap, cap), col(c)] = dot(hidden(s, 1, j), down_v[j, :, col(c)]).astype(BF)
        ret_copy(s, c, col).start()

    def weave(s):
        table = cols[s]
        spot = lax.broadcasted_iota(jnp.int32, (rows_all, cap), 1).astype(F32)
        for e in range(2 * local):
            here = spot == table[:, e:e + 1]
            comb[s, :, pl.ds(e * cap, cap)] = jnp.where(here, table[:, 16 + e:17 + e], 0.0).astype(BF)

    def mix(s, c, put):
        ret_copy(s, c, col).wait_recv()

        @pl.loop(0, 2)
        def _(k):
            group = pl.ds(pl.multiple_of(k * (rows_all // 2), rows_all // 2), rows_all // 2)
            near = dot(comb[s, group, pl.ds(0, count)], out_o[s, :, col(c)])
            put(group, near + dot(comb[s, group, pl.ds(count, count)], ret_r[s, :, col(c)]))

    def stage_d(s, c, more):
        if more:
            sum_wait(block(s), c, col)

        def put(group, total):
            if more:
                total = total + sum_r[block(s), group, col(c)].astype(F32)
            sum_s[s - 1, group, col(c)] = total.astype(BF)

        mix(s, c, put)
        sum_copy(s, c, col).start()

    def own_mix(c):
        def put(group, total):
            acc[group, col(c)] = total

        mix(0, c, put)

    def add_spare(c):
        sum_wait(spare, c, col)
        acc[:, col(c)] += sum_r[spare, :, col(c)].astype(F32)

    def add_last(c):
        sum_wait(z, c, col)
        acc[:, col(c)] += sum_r[z, :, col(c)].astype(F32)

    def pass_on(s, c):
        relay(s, c).wait_recv()
        relay(s, c).start()

    def pass_note(s):
        relay_note(s).wait_recv()
        relay_note(s).start()

    def arrive(s, c):
        relay(s, c).wait_recv()

    def take_note(s):
        relay_note(s).wait_recv()

    def lead(k):
        own_copy(0, k).start()

    def run(order, at_end):
        def prep(s):
            if at_end:
                take_note(s)
            prepare(s)

        def bring(s, c):
            if at_end:
                arrive(s, c)
            pack(s, c)

        calls = {
            "passn": pass_note, "pass": pass_on, "ownin": lead, "prep": prep, "pack": bring,
            "a": stage_a, "b": stage_b, "c": stage_c, "c1": send_back, "weave": weave, "mix0": own_mix,
            "d": lambda s, c: stage_d(s, c, not at_end), "spare": add_spare, "last": add_last,
        }
        for name, *where in order:
            calls[name](*where)

    pl.semaphore_wait(barrier, jnp.where(inner, 3, 2) + nt - 1)
    x_loads[0].wait()
    own_copy(0, 0).start()

    @pl.when(inner)
    def _():
        own_copy(1, 0).start()

    for load in x_loads[1:]:
        load.wait()
    values = x_ref[...].astype(F32)
    start_sum(0, jnp.sum(values * values, axis=1, keepdims=True))
    send_sum(0)
    shape = (rows_all, rows_all)
    earlier = lax.broadcasted_iota(jnp.int32, shape, 0) < lax.broadcasted_iota(jnp.int32, shape, 1)
    tri[...] = jnp.where(earlier, 1.0, 0.0).astype(BF)
    for load in small_loads:
        load.wait()
    blank = jnp.zeros((3, rows_all), F32)
    note_s[...] = jnp.concatenate(
        [route_ref[...].astype(F32), weight_ref[...], finish_sum(0)[0:1], blank], axis=0
    )
    own_note(0).start()

    @pl.when(inner)
    def _():
        own_note(1).start()
        for c in range(1, parts // 2):
            own_copy(0, c).start()
        for c in range(1, parts):
            own_copy(1, c).start()

    @pl.when(end)
    def _():
        for c in range(1, parts):
            own_copy(0, c).start()

    prepare(0)
    for c in range(parts):
        pack(0, c)
    for load in loads:
        load.wait()

    @pl.when(end)
    def _():
        run(END_ORDER, True)

    @pl.when(inner)
    def _():
        run(INNER_ORDER, False)

    summed = acc[...]
    start_sum(1, jnp.sum(summed * summed, axis=1, keepdims=True))
    send_sum(1)

    for i in range(2 * last + 2):
        for o in range(1, nt):
            p_copy(i, o).wait_send()
            h_copy(i, o).wait_send()
    for s in range(last + 1):
        for c in range(parts):
            pack_copy(s, c).wait_send()
            ret_copy(s, c, col).wait_send()
            if s:
                sum_copy(s, c, col).wait_send()
    for c in range(parts):
        own_copy(0, c).wait_send()
    own_note(0).wait_send()

    @pl.when(inner)
    def _():
        own_note(1).wait_send()
        for c in range(parts):
            own_copy(1, c).wait_send()
        for s in range(1, last + 1):
            relay_note(s).wait_send()
            for c in range(parts):
                relay(s, c).wait_send()

    scale = jnp.sum(jnp.where(eye(), finish_sum(1)[0:1], 0.0), axis=1, keepdims=True)
    out_ref[...] = (acc[...] * scale * last_gain_ref[...]).astype(BF)
    for k in range(2):
        for o in range(1, nt):
            sq_copy(k, o).wait_send()


def line_call(n, nt, local, cap, full, tokens, routes, weights, norm_gain, gate_weight, up_weight, down_weight, final_gain):
    rows, width = tokens.shape
    ff = gate_weight.shape[2]
    line = n // 2
    count = local * cap
    parts = 4
    any_spec = pl.BlockSpec(memory_space=pltpu.HBM)
    vmem = pl.BlockSpec(memory_space=pltpu.VMEM)
    dma = pltpu.SemaphoreType.DMA
    return pl.pallas_call(
        functools.partial(line_kernel, n, nt, local, cap, full, parts),
        out_shape=jax.ShapeDtypeStruct((rows, width), BF),
        in_specs=[any_spec, any_spec, any_spec, any_spec, any_spec, any_spec, any_spec, any_spec],
        out_specs=vmem,
        scratch_shapes=[
            pltpu.VMEM(gate_weight.shape, BF),
            pltpu.VMEM(up_weight.shape, BF),
            pltpu.VMEM(down_weight.shape, BF),
            pltpu.VMEM(routes.T.shape, routes.dtype),
            pltpu.VMEM(weights.T.shape, F32),
            pltpu.VMEM((1, width), F32),
            pltpu.VMEM((1, width), F32),
            pltpu.VMEM((rows, width), BF),
            pltpu.VMEM((line, rows, width), BF),
            pltpu.VMEM((line, 8, rows), F32),
            pltpu.VMEM((8, rows), F32),
            pltpu.VMEM((rows, rows), BF),
            pltpu.VMEM((line, rows, 128), F32),
            pltpu.VMEM((2 * count, rows), BF),
            pltpu.VMEM((2 * count, 128), F32),
            pltpu.VMEM((line, 2 * count, width), BF),
            pltpu.VMEM((line, count, width), BF),
            pltpu.VMEM((n, nt, count, 2 * ff // nt), BF),
            pltpu.VMEM((n, nt - 1, count, 2 * ff // nt), BF),
            pltpu.VMEM((n, nt, count, ff // nt), BF),
            pltpu.VMEM((line, count, width), BF),
            pltpu.VMEM((line, count, width), BF),
            pltpu.VMEM((line, count, width), BF),
            pltpu.VMEM((line, rows, 2 * count), BF),
            pltpu.VMEM((line - 1, rows, width), BF),
            pltpu.VMEM((line + 1, rows, width), BF),
            pltpu.VMEM((rows, width), F32),
            pltpu.VMEM((2, 8, rows), F32),
            pltpu.VMEM((2, nt - 1, 8, rows), F32),
            dma((3,)),
            dma((4,)),
            dma((parts,)),
            dma((2, parts)),
            dma((line - 1, parts)),
            dma((line, parts)),
            dma((2,)),
            dma((line - 1,)),
            dma((line,)),
            dma((line, parts)),
            dma((line, parts)),
            dma((n, nt - 1)),
            dma((n, nt - 1)),
            dma((n, nt - 1)),
            dma((n, nt - 1)),
            dma((line, parts)),
            dma((line, parts)),
            dma((line - 1, parts)),
            dma((line + 1, parts)),
            dma((2, nt - 1)),
            dma((2, nt - 1)),
        ],
        compiler_params=pltpu.CompilerParams(
            collective_id=0, has_side_effects=True, vmem_limit_bytes=62 * 1024 * 1024
        ),
    )(tokens, routes.T, weights.T, norm_gain[None], final_gain[None], gate_weight, up_weight, down_weight)


RING_BYTES = 24 * 1024 * 1024


def body(tokens, routes, route_weights, norm_gain, gate_weight, up_weight, down_weight, final_gain):
    n, nt = lax.axis_size("ep"), lax.axis_size("tp")
    local, width, ff = gate_weight.shape
    experts = n * local
    rows = tokens.shape[0]
    full = width * nt
    cap = 4 * rows // experts
    count = local * cap
    blocks = max(n - 4, 0)
    ring = n % 2 == 0 and n >= 6 and local % 2 == 0 and blocks * rows * width * 2 <= RING_BYTES
    if n == 8 and local <= 8 and width % 512 == 0 and cap % 128 == 0:
        return line_call(
            n, nt, local, cap, full, tokens, routes, route_weights, norm_gain, gate_weight, up_weight, down_weight, final_gain
        )
    meta = jnp.concatenate(
        [routes.T.astype(F32), route_weights.T, jnp.zeros((4, rows), F32)], axis=0
    )
    tables = 1 + blocks if ring else 1
    packed = count + local // 2 * cap

    any_spec = pl.BlockSpec(memory_space=pl.ANY)
    vmem = pl.BlockSpec(memory_space=pltpu.VMEM)
    dma = pltpu.SemaphoreType.DMA

    def only(ring_shape, shape, kind=BF):
        return pltpu.VMEM(ring_shape if ring else shape, kind)

    tiny = (1, 16, 128)
    return pl.pallas_call(
        functools.partial(kernel, n, nt, local, cap, ring, full),
        out_shape=jax.ShapeDtypeStruct((rows, width), BF),
        in_specs=[vmem, vmem, vmem, vmem, any_spec, any_spec, any_spec],
        out_specs=vmem,
        scratch_shapes=[
            pltpu.VMEM(gate_weight.shape, BF),
            pltpu.VMEM(up_weight.shape, BF),
            pltpu.VMEM(down_weight.shape, BF),
            pltpu.VMEM((rows, width), BF),
            pltpu.VMEM((rows, width), F32),
            pltpu.VMEM((rows, rows), BF),
            pltpu.VMEM((tables, experts, rows), F32),
            pltpu.VMEM((tables, experts, rows), F32),
            pltpu.VMEM((2, 8, rows), F32),
            pltpu.VMEM((2, nt - 1, 8, rows), F32),
            only(tiny, (n, count, width)),
            only((blocks, rows, width), (n, count, width)),
            only((2, packed, width), tiny),
            only((2, packed, width), tiny),
            only((2, local // 2 * cap, width), tiny),
            only((blocks, 8, rows), (1, 8, 128), F32),
            pltpu.VMEM((n, nt, count, 2 * ff // nt), BF),
            pltpu.VMEM((n, nt - 1, count, 2 * ff // nt), BF),
            pltpu.VMEM((n, nt, count, ff // nt), BF),
            pltpu.VMEM((n, count, width), BF),
            pltpu.VMEM((n, count, width), BF),
            dma((3,)),
            dma((blocks, 2) if ring else (n,)),
            dma((blocks, 2) if ring else (n,)),
            dma((2,)),
            dma((2,)),
            dma((2,)),
            dma((2,)),
            dma((blocks,) if ring else (1,)),
            dma((blocks,) if ring else (1,)),
            dma((n, nt - 1)),
            dma((n, nt - 1)),
            dma((n, nt - 1)),
            dma((n, nt - 1)),
            dma((n,)),
            dma((n,)),
            dma((2, nt - 1)),
            dma((2, nt - 1)),
        ],
        compiler_params=pltpu.CompilerParams(
            collective_id=0, has_side_effects=True, vmem_limit_bytes=60 * 1024 * 1024
        ),
    )(tokens, meta, norm_gain[None], final_gain[None], gate_weight, up_weight, down_weight)


def solution(mesh):
    in_specs = (
        P("ep", "tp"),
        P("ep", None),
        P("ep", None),
        P("tp"),
        P("ep", "tp", None),
        P("ep", "tp", None),
        P("ep", None, "tp"),
        P("tp"),
    )
    return jax.shard_map(body, mesh=mesh, in_specs=in_specs, out_specs=P("ep", "tp"), check_vma=False)
```

```python
import functools

import jax
import jax.numpy as jnp
from jax import lax
from jax.experimental import pallas as pl
from jax.experimental.pallas import tpu as pltpu
from jax.sharding import PartitionSpec as P

EPSILON = 1e-06
BF = jnp.bfloat16
F32 = jnp.float32


def dot(a, b):
    return jnp.dot(a, b, preferred_element_type=F32)


def dot_t(a, b):
    return lax.dot_general(a, b, (((0,), (0,)), ((), ())), preferred_element_type=F32)


def kernel(
    n, nt, local, cap, ring, full,
    x_ref, meta_ref, gain_ref, last_gain_ref, gate_hbm, up_hbm, down_hbm, out_ref,
    gate_v, up_v, down_v, xn, acc, tri, rank_t, wt_t, sq, sq2,
    send_x, recv_x, pk_s, pk_r, far_r, meta_r,
    part, recv_p, hid, out_s, out_r,
    w_sem, xs_sem, xr_sem, ks_sem, kr_sem, fs_sem, fr_sem, ms_sem, mr_sem,
    ps_sem, pr_sem, hs_sem, hr_sem, os_sem, or_sem, qs_sem, qr_sem,
):
    me = lax.axis_index("ep")
    my_tp = lax.axis_index("tp")
    ff = gate_v.shape[2]
    fq = ff // nt
    rows_all = x_ref.shape[0]
    half = n // 2
    chunk = rows_all // 2
    count = local * cap
    split = local // 2

    loads = [
        pltpu.make_async_copy(src, dst, w_sem.at[i])
        for i, (src, dst) in enumerate(((gate_hbm, gate_v), (up_hbm, up_v), (down_hbm, down_v)))
    ]
    for load in loads:
        load.start()

    barrier = pltpu.get_barrier_semaphore()

    @pl.loop(1, n)
    def _(s):
        pl.semaphore_signal(barrier, inc=1, device_id={"ep": lax.rem(me + s, n), "tp": my_tp})

    for o in range(1, nt):
        pl.semaphore_signal(barrier, inc=1, device_id={"ep": me, "tp": lax.rem(my_tp + o, nt)})

    place = jnp.where(me % 2 == 0, me // 2, n - 1 - me // 2)

    def at_place(p):
        p = lax.rem(p + 2 * n, n)
        return jnp.where(p < half, 2 * p, 2 * (n - 1 - p) + 1)

    def shift(s):
        return (1 - 2 * ((s + 1) % 2)) * ((s + 1) // 2)

    def source(s):
        if ring:
            return at_place(place - shift(s))
        return lax.rem(me - s + n, n)

    def sender(s):
        if ring:
            return at_place(place + shift(s))
        return lax.rem(me + s, n)

    def eye():
        shape = (rows_all, rows_all)
        return lax.broadcasted_iota(jnp.int32, shape, 0) == lax.broadcasted_iota(jnp.int32, shape, 1)

    def sq_copy(k, o):
        q = lax.rem(my_tp + o, nt)
        return pltpu.make_async_remote_copy(
            sq.at[k], sq2.at[k, o - 1], qs_sem.at[k, o - 1], qr_sem.at[k, o - 1],
            device_id={"ep": me, "tp": q},
        )

    def start_sum(k, column):
        row = jnp.sum(jnp.where(eye(), column, 0.0), axis=0, keepdims=True)
        sq[k] = jnp.broadcast_to(row, sq.shape[1:])

    def send_sum(k):
        for o in range(1, nt):
            sq_copy(k, o).start()

    def finish_sum(k):
        for o in range(1, nt):
            sq_copy(k, o).wait_recv()
        total = sq[k]
        for o in range(1, nt):
            total = total + sq2[k, o - 1]
        scale = lax.rsqrt(total[0:1] / full + EPSILON)
        return jnp.sum(jnp.where(eye(), scale, 0.0), axis=1, keepdims=True)

    def make_table(slot, meta):
        names = lax.broadcasted_iota(jnp.int32, rank_t.shape[1:], 0).astype(F32)
        first, second = meta[0:1] == names, meta[1:2] == names
        hit = first | second
        before = dot(jnp.where(hit, 1.0, 0.0).astype(BF), tri[...])
        rank_t[slot] = jnp.where(hit, before, -1.0)
        wt_t[slot] = jnp.where(first, meta[2:3], 0.0) + jnp.where(second, meta[3:4], 0.0)

    def onehot(slot, expert, weighted=False):
        rank = rank_t[slot, pl.ds(expert, 1), :]
        hit = lax.broadcasted_iota(jnp.int32, (cap, rows_all), 0).astype(F32) == rank
        return jnp.where(hit, wt_t[slot, pl.ds(expert, 1), :] if weighted else F32(1.0), F32(0.0))

    def pack(slot, experts, block):
        pick = jnp.concatenate([onehot(slot, e) for e in experts], axis=0).astype(BF)
        return dot(pick, block).astype(BF)

    def experts_of(owner):
        return [owner * local + j for j in range(local)]

    def x_copy(s):
        return pltpu.make_async_remote_copy(
            send_x.at[s], recv_x.at[s], xs_sem.at[s], xr_sem.at[s],
            device_id={"ep": sender(s), "tp": my_tp},
        )

    def ahead(i):
        return {"ep": at_place(place + 1 - 2 * i), "tp": my_tp}

    def block_copy(d, i, k):
        piece = pl.ds(k * chunk, chunk)
        src = xn.at[piece] if d == 1 else recv_x.at[2 * d - 4 + i, piece]
        slot = 2 * d - 2 + i
        return pltpu.make_async_remote_copy(
            src, recv_x.at[slot, piece], xs_sem.at[slot, k], xr_sem.at[slot, k], device_id=ahead(i)
        )

    def meta_copy(d, i):
        slot = 2 * d - 2 + i
        return pltpu.make_async_remote_copy(
            meta_ref if d == 1 else meta_r.at[slot - 2], meta_r.at[slot],
            ms_sem.at[slot], mr_sem.at[slot], device_id=ahead(i),
        )

    def pack_copy(i):
        return pltpu.make_async_remote_copy(
            pk_s.at[i], pk_r.at[i], ks_sem.at[i], kr_sem.at[i], device_id=ahead(i)
        )

    def far_copy(i):
        return pltpu.make_async_remote_copy(
            pk_r.at[i, pl.ds(count, split * cap)], far_r.at[i], fs_sem.at[i], fr_sem.at[i],
            device_id=ahead(i),
        )

    def p_copy(s, o):
        q = lax.rem(my_tp + o, nt)
        return pltpu.make_async_remote_copy(
            part.at[s, q], recv_p.at[s, o - 1], ps_sem.at[s, o - 1], pr_sem.at[s, o - 1],
            device_id={"ep": me, "tp": q},
        )

    def h_copy(s, o, back=False):
        mine = lax.rem(my_tp - o + nt, nt) if back else my_tp
        q = lax.rem(my_tp - o + nt, nt) if back else lax.rem(my_tp + o, nt)
        return pltpu.make_async_remote_copy(
            hid.at[s, mine], hid.at[s, mine], hs_sem.at[s, o - 1], hr_sem.at[s, o - 1],
            device_id={"ep": me, "tp": q},
        )

    def o_copy(s):
        return pltpu.make_async_remote_copy(
            out_s.at[s], out_r.at[s], os_sem.at[s], or_sem.at[s],
            device_id={"ep": source(s), "tp": my_tp},
        )

    def stage_a(s, rows_of):
        for j in range(local):
            rows = rows_of(j)
            gate = dot(rows, gate_v[j]).astype(BF)
            upper = dot(rows, up_v[j]).astype(BF)
            for q in range(nt):
                part[s, q, pl.ds(j * cap, cap), pl.ds(0, fq)] = gate[:, q * fq:(q + 1) * fq]
                part[s, q, pl.ds(j * cap, cap), pl.ds(fq, fq)] = upper[:, q * fq:(q + 1) * fq]
        for o in range(1, nt):
            p_copy(s, o).start()

    def stage_b(s):
        for o in range(1, nt):
            p_copy(s, o).wait_recv()
        total = part[s, my_tp].astype(F32)
        for o in range(1, nt):
            total = total + recv_p[s, o - 1].astype(F32)
        gate, upper = total[:, :fq], total[:, fq:]
        hid[s, my_tp] = (gate / (1.0 + jnp.exp(-gate)) * upper).astype(BF)
        for o in range(1, nt):
            h_copy(s, o).start()

    def stage_c(s, own):
        for o in range(1, nt):
            h_copy(s, o, True).wait_recv()
        target = out_r if own else out_s
        for j in range(local):
            hidden = jnp.concatenate([hid[s, q, pl.ds(j * cap, cap), :] for q in range(nt)], axis=1)
            target[s, pl.ds(j * cap, cap), :] = dot(hidden, down_v[j]).astype(BF)
        if not own:
            o_copy(s).start()

    def combine(s):
        weight = jnp.concatenate([onehot(0, e, True) for e in experts_of(sender(s))], axis=0)
        high = weight.astype(BF)
        low = (weight - high.astype(F32)).astype(BF)
        rows = out_r[s]
        return dot_t(high, rows) + dot_t(low, rows)

    values = x_ref[...].astype(F32)
    start_sum(0, jnp.sum(values * values, axis=1, keepdims=True))
    shape = (rows_all, rows_all)
    earlier = lax.broadcasted_iota(jnp.int32, shape, 0) < lax.broadcasted_iota(jnp.int32, shape, 1)
    tri[...] = jnp.where(earlier, 1.0, 0.0).astype(BF)
    pl.semaphore_wait(barrier, n - 1 + nt - 1)
    send_sum(0)
    if ring:
        for i in range(2):
            meta_copy(1, i).start()
    make_table(0, meta_ref[...])
    scale = finish_sum(0)
    xn[...] = (x_ref[...].astype(F32) * scale * gain_ref[...]).astype(BF)

    def own_rows(j):
        return pack(0, [me * local + j], xn[...])

    def stored(ref, slot):
        return lambda j: ref[slot, pl.ds(j * cap, cap), :]

    if ring:
        for k in range(2):
            for i in range(2):
                block_copy(1, i, k).start()
        for load in loads:
            load.wait()
        stage_a(0, own_rows)
        for d in range(1, half + 1):
            if d <= half - 2:
                for k in range(2):
                    for i in range(2):
                        block_copy(d, i, k).wait_recv()
                        if d < half - 2:
                            block_copy(d + 1, i, k).start()
                for i in range(2):
                    slot = 2 * d - 2 + i
                    meta_copy(d, i).wait_recv()
                    if d < half - 2:
                        meta_copy(d + 1, i).start()
                    make_table(1 + slot, meta_r[slot])
                if d == half - 2:
                    for i in range(2):
                        slot = 2 * d - 2 + i
                        step = 1 - 2 * i
                        far = experts_of(at_place(place + 2 * step))
                        wanted = experts_of(at_place(place + step)) + (far[split:] if i else far[:split])
                        pk_s[i] = pack(1 + slot, wanted, recv_x[slot])
                        pack_copy(i).start()
            elif d == half - 1:
                for i in range(2):
                    pack_copy(i).wait_recv()
                    far_copy(i).start()
            else:
                for i in range(2):
                    far_copy(i).wait_recv()
            for i in range(2 if d < half else 1):
                s = 2 * d - 1 + i
                slot = s - 1
                if d <= half - 2:
                    stage_a(s, lambda j, slot=slot: pack(1 + slot, [me * local + j], recv_x[slot]))
                elif d == half - 1:
                    stage_a(s, stored(pk_r, i))
                else:
                    stage_a(s, lambda j: far_r[j // split, pl.ds(j % split * cap, cap), :])
                stage_b(s - 1)
                if s >= 2:
                    stage_c(s - 2, s == 2)
    else:
        send_x[1] = pack(0, experts_of(sender(1)), xn[...])

        @pl.loop(2, n)
        def _(s):
            send_x[s] = pack(0, experts_of(sender(s)), xn[...])
            x_copy(s - 1).start()

        for load in loads:
            load.wait()
        stage_a(0, own_rows)
        x_copy(n - 1).start()
        x_copy(1).wait_recv()
        stage_a(1, stored(recv_x, 1))
        stage_b(0)
        x_copy(2).wait_recv()
        stage_a(2, stored(recv_x, 2))
        stage_b(1)
        stage_c(0, True)

        @pl.loop(3, n)
        def _(s):
            x_copy(s).wait_recv()
            stage_a(s, stored(recv_x, s))
            stage_b(s - 1)
            stage_c(s - 2, False)

    stage_b(n - 1)
    stage_c(n - 2, False)
    acc[...] = combine(0)
    stage_c(n - 1, False)

    @pl.loop(1, n)
    def _(s):
        o_copy(s).wait_recv()
        acc[...] += combine(s)

    summed = acc[...]
    start_sum(1, jnp.sum(summed * summed, axis=1, keepdims=True))

    @pl.loop(0, n)
    def _(s):
        for o in range(1, nt):
            p_copy(s, o).wait_send()
            h_copy(s, o).wait_send()

    send_sum(1)

    @pl.loop(1, n)
    def _(s):
        o_copy(s).wait_send()

    if ring:
        for i in range(2):
            for d in range(1, half - 1):
                meta_copy(d, i).wait_send()
                for k in range(2):
                    block_copy(d, i, k).wait_send()
            pack_copy(i).wait_send()
            far_copy(i).wait_send()
    else:
        @pl.loop(1, n)
        def _(s):
            x_copy(s).wait_send()

    scale = finish_sum(1)
    out_ref[...] = (acc[...] * scale * last_gain_ref[...]).astype(BF)
    for k in range(2):
        for o in range(1, nt):
            sq_copy(k, o).wait_send()


END_ORDER = (
    ("prep", 1), ("a", 0, 0), ("pack", 1, 0), ("pack", 1, 1), ("weave", 1), ("pack", 1, 2), ("pack", 1, 3),
    ("a", 1, 0), ("a2", 1, 0), ("weave", 0), ("a", 0, 1), ("a", 1, 1), ("a2", 1, 1), ("b", 1, 0), ("prep", 2),
    ("pack", 2, 0), ("pack", 2, 1), ("a2", 0, 0), ("b", 1, 1), ("weave", 2), ("a2", 0, 1), ("pack", 2, 2),
    ("c1", 1, 0), ("pack", 2, 3), ("a", 2, 0), ("c1", 1, 1), ("c", 1), ("b", 0, 1), ("b", 0, 0), ("d", 1, 0),
    ("c1", 1, 2), ("a", 2, 1), ("a2", 2, 1), ("d", 1, 1), ("a2", 2, 0), ("prep", 3), ("pack", 3, 0), ("b", 2,
    1), ("d", 1, 2), ("pack", 3, 1), ("pack", 3, 2), ("b", 2, 0), ("c1", 2, 0), ("pack", 3, 3), ("a", 3, 0),
    ("c", 2), ("d", 2, 0), ("c1", 2, 1), ("c1", 0, 0), ("c1", 2, 2), ("c1", 2, 3), ("a2", 3, 0), ("a", 3, 1),
    ("a2", 3, 1), ("d", 2, 1), ("b", 3, 1), ("c", 0), ("c1", 0, 1), ("d", 2, 2), ("mix0", 0), ("weave", 3),
    ("c1", 3, 0), ("c1", 3, 1), ("c1", 3, 2), ("d", 2, 3), ("b", 3, 0), ("c", 3), ("d", 3, 0), ("mix0", 1),
    ("c1", 0, 2), ("c1", 3, 3), ("d", 3, 2), ("c1", 0, 3), ("last", 1), ("d", 3, 1), ("d", 3, 3), ("mix0", 2),
    ("last", 2), ("c1", 1, 3), ("mix0", 3), ("last", 0), ("last", 3), ("d", 1, 3),
)

INNER_ORDER = (
    ("a", 0, 0), ("passn", 1), ("prep", 1), ("pass", 1, 0), ("passn", 3), ("a", 0, 1), ("a2", 0, 1), ("pass",
    2, 0), ("pass", 1, 1), ("pack", 1, 0), ("pack", 1, 1), ("pass", 1, 2), ("pass", 1, 3), ("pack", 1, 2),
    ("pack", 1, 3), ("passn", 2), ("a", 1, 0), ("a2", 1, 0), ("a2", 0, 0), ("pass", 2, 1), ("pass", 2, 2),
    ("ownin", 2), ("b", 0, 1), ("a", 1, 1), ("a2", 1, 1), ("prep", 2), ("pack", 2, 0), ("pack", 2, 1),
    ("pack", 2, 2), ("pass", 2, 3), ("pass", 3, 0), ("b", 1, 0), ("ownin", 3), ("pack", 2, 3), ("prep", 3),
    ("a", 2, 0), ("pack", 3, 0), ("pass", 3, 1), ("pack", 3, 1), ("a2", 2, 0), ("b", 1, 1), ("weave", 0),
    ("pass", 3, 2), ("b", 2, 0), ("a", 2, 1), ("a2", 2, 1), ("c", 1), ("pass", 3, 3), ("pack", 3, 2), ("pack",
    3, 3), ("b", 2, 1), ("weave", 2), ("a", 3, 0), ("c1", 0, 0), ("c1", 0, 1), ("c", 2), ("c1", 0, 2), ("a2",
    3, 0), ("a", 3, 1), ("c1", 0, 3), ("b", 3, 0), ("c1", 1, 0), ("c1", 2, 0), ("weave", 1), ("c1", 2, 1),
    ("c1", 2, 2), ("c1", 1, 1), ("c1", 1, 2), ("c1", 2, 3), ("a2", 3, 1), ("c", 3), ("b", 0, 0), ("d", 2, 0),
    ("b", 3, 1), ("d", 2, 1), ("c1", 1, 3), ("weave", 3), ("c", 0), ("mix0", 0), ("d", 1, 0), ("d", 2, 2),
    ("mix0", 3), ("mix0", 1), ("c1", 3, 0), ("spare", 0), ("d", 1, 1), ("c1", 3, 1), ("c1", 3, 2), ("spare",
    1), ("d", 2, 3), ("d", 1, 2), ("d", 3, 0), ("d", 1, 3), ("d", 3, 2), ("d", 3, 1), ("c1", 3, 3), ("d", 3,
    3), ("mix0", 2), ("spare", 2), ("last", 2), ("last", 0), ("spare", 3), ("last", 1), ("last", 3),
)


def line_kernel(
    n, nt, local, cap, full, parts,
    x_hbm, route_hbm, weight_hbm, gain_hbm, last_gain_hbm, gate_hbm, up_hbm, down_hbm, out_hbm,
    gate_v, up_v, down_v, route_ref, weight_ref, gain_ref, last_gain_ref, x_ref, xs, notes, note_s, tri, cols, pick, lift, pk_s, pk_r,
    part, recv_p, pair_s, pair_r, hid, out_o, ret_s, ret_r, comb, sum_s, sum_r, acc, sq, sq2,
    w_sem, small_sem, x_sem, own_sem, rel_sem, blk_sem, nown_sem, nrel_sem, note_sem, ks_sem, kr_sem,
    ps_sem, pr_sem, ys_sem, yr_sem, hs_sem, hr_sem, ts_sem, tr_sem, ss_sem, sr_sem, qs_sem, qr_sem,
):
    me = lax.axis_index("ep")
    my_tp = lax.axis_index("tp")
    ff = gate_v.shape[2]
    fq = ff // nt
    rows_all, width = x_ref.shape
    cw = width // parts
    count = local * cap
    last = n // 2 - 1
    z, side = me // 2, me % 2
    low = z <= last // 2
    inner = (z >= 1) & (z <= last - 1)
    end = jnp.logical_not(inner)
    step_in = jnp.where(low, 2, -2)
    inward = {"ep": me + step_in, "tp": my_tp}
    outward = {"ep": jnp.where(inner, me - step_in, me + step_in), "tp": my_tp}
    mate = me + 1 - 2 * side
    across = {"ep": mate, "tp": my_tp}
    spare = last + 1
    pair, row = my_tp % 2, my_tp // 2
    partner, facing = my_tp + 1 - 2 * pair, lax.rem(my_tp + 2, nt)

    def block(s):
        if s == 0:
            return z
        near = jnp.where(inner, 0, 1) if s == 1 else (last if s == 2 else last - 1)
        return jnp.where(low, near, last - near)

    loads = [
        pltpu.make_async_copy(src, dst, w_sem.at[i])
        for i, (src, dst) in enumerate(((gate_hbm, gate_v), (up_hbm, up_v), (down_hbm, down_v)))
    ]
    x_loads = [
        pltpu.make_async_copy(x_hbm.at[:, pl.ds(c * cw, cw)], x_ref.at[:, pl.ds(c * cw, cw)], x_sem.at[c])
        for c in range(parts)
    ]
    small = ((route_hbm, route_ref), (weight_hbm, weight_ref), (gain_hbm, gain_ref), (last_gain_hbm, last_gain_ref))
    small_loads = [pltpu.make_async_copy(src, dst, small_sem.at[i]) for i, (src, dst) in enumerate(small)]
    for load in x_loads + small_loads + loads:
        load.start()

    barrier = pltpu.get_barrier_semaphore()
    pl.semaphore_signal(barrier, inc=1, device_id=inward)
    pl.semaphore_signal(barrier, inc=1, device_id=across)

    @pl.when(inner)
    def _():
        pl.semaphore_signal(barrier, inc=1, device_id=outward)

    for o in range(1, nt):
        pl.semaphore_signal(barrier, inc=1, device_id={"ep": me, "tp": lax.rem(my_tp + o, nt)})

    def col(c):
        return pl.ds(c * cw, cw)

    def dcol(c):
        return pl.ds(pl.multiple_of(c * cw, cw), cw)

    def eye():
        shape = (rows_all, rows_all)
        return lax.broadcasted_iota(jnp.int32, shape, 0) == lax.broadcasted_iota(jnp.int32, shape, 1)

    def sq_copy(k, o):
        q = lax.rem(my_tp + o, nt)
        return pltpu.make_async_remote_copy(
            sq.at[k], sq2.at[k, o - 1], qs_sem.at[k, o - 1], qr_sem.at[k, o - 1],
            device_id={"ep": me, "tp": q},
        )

    def start_sum(k, column):
        row = jnp.sum(jnp.where(eye(), column, 0.0), axis=0, keepdims=True)
        sq[k] = jnp.broadcast_to(row, sq.shape[1:])

    def send_sum(k):
        for o in range(1, nt):
            sq_copy(k, o).start()

    def finish_sum(k):
        for o in range(1, nt):
            sq_copy(k, o).wait_recv()
        total = sq[k]
        for o in range(1, nt):
            total = total + sq2[k, o - 1]
        return lax.rsqrt(total / full + EPSILON)

    def own_copy(d, c):
        return pltpu.make_async_remote_copy(
            x_ref.at[:, col(c)], xs.at[z, :, col(c)], own_sem.at[d, c], blk_sem.at[z, c],
            device_id=outward if d else inward,
        )

    def relay(s, c):
        b = block(s)
        return pltpu.make_async_remote_copy(
            xs.at[b, :, col(c)], xs.at[b, :, col(c)], rel_sem.at[s - 1, c], blk_sem.at[b, c],
            device_id=inward if s == 1 else outward,
        )

    def own_note(d):
        return pltpu.make_async_remote_copy(
            note_s, notes.at[z], nown_sem.at[d], note_sem.at[z], device_id=outward if d else inward
        )

    def relay_note(s):
        b = block(s)
        return pltpu.make_async_remote_copy(
            notes.at[b], notes.at[b], nrel_sem.at[s - 1], note_sem.at[b],
            device_id=inward if s == 1 else outward,
        )

    def pack_copy(s, c):
        return pltpu.make_async_remote_copy(
            pk_s.at[s, pl.ds(count, count), col(c)], pk_r.at[s, :, col(c)], ks_sem.at[s, c], kr_sem.at[s, c],
            device_id=across,
        )

    def ret_copy(s, c, at):
        return pltpu.make_async_remote_copy(
            ret_s.at[s, :, at(c)], ret_r.at[s, :, at(c)], ts_sem.at[s, c], tr_sem.at[s, c],
            device_id=across,
        )

    def sum_copy(s, c, at):
        slot = jnp.where(end, spare, block(s)) if s == 1 else block(s)
        ep = jnp.where(inner, outward["ep"], inward["ep"]) if s == 1 else inward["ep"]
        return pltpu.make_async_remote_copy(
            sum_s.at[s - 1, :, at(c)], sum_r.at[slot, :, at(c)], ss_sem.at[s - 1, c], sr_sem.at[slot, c],
            device_id={"ep": ep, "tp": my_tp},
        )

    def sum_wait(slot, c, at):
        pltpu.make_async_remote_copy(
            sum_s.at[0, :, at(c)], sum_r.at[slot, :, at(c)], ss_sem.at[0, c], sr_sem.at[slot, c],
            device_id=inward,
        ).wait_recv()

    def p_copy(i):
        return pltpu.make_async_remote_copy(
            part.at[i, pl.ds(2 * (1 - pair), 2)], recv_p.at[i], ps_sem.at[i], pr_sem.at[i],
            device_id={"ep": me, "tp": partner},
        )

    def y_copy(i):
        return pltpu.make_async_remote_copy(
            pair_s.at[i], pair_r.at[i], ys_sem.at[i], yr_sem.at[i], device_id={"ep": me, "tp": facing}
        )

    def h_copy(i, o, back=False):
        mine = lax.rem(my_tp - o + nt, nt) if back else my_tp
        q = lax.rem(my_tp - o + nt, nt) if back else lax.rem(my_tp + o, nt)
        return pltpu.make_async_remote_copy(
            hid.at[i, mine], hid.at[i, mine], hs_sem.at[i, o - 1], hr_sem.at[i, o - 1],
            device_id={"ep": me, "tp": q},
        )

    def prepare(s):
        meta = notes[block(s)] if s else note_s[...]
        row = lax.broadcasted_iota(jnp.int32, (16, rows_all), 0)
        name = jnp.where(row < local, me * local + row, mate * local + row - local)
        name = jnp.where(row < 2 * local, name, -1).astype(F32)
        first, second = meta[0:1] == name, meta[1:2] == name
        hit = first | second
        before = dot(jnp.where(hit, 1.0, 0.0).astype(BF), tri[...])
        rank = jnp.where(hit, before, -1.0)
        weight = jnp.where(first, meta[2:3], 0.0) + jnp.where(second, meta[3:4], 0.0)
        blank = jnp.zeros((128 - 32, rows_all), F32)
        cols[s] = jnp.concatenate([rank, weight, blank], axis=0).T
        spot = lax.broadcasted_iota(jnp.int32, (cap, rows_all), 0).astype(F32)
        for e in range(2 * local):
            at = pl.ds(e * cap, cap)
            here = spot == rank[e:e + 1]
            pick[at, :] = jnp.where(here, 1.0, 0.0).astype(BF)
            total = jnp.sum(jnp.where(here, meta[4:5], 0.0), axis=1, keepdims=True)
            lift[at, :] = jnp.broadcast_to(total, (cap, lift.shape[1]))

    def pack(s, c):
        values = x_ref.at[:, col(c)] if s == 0 else xs.at[block(s), :, col(c)]

        def groups(first):
            @pl.loop(first, first + local)
            def _(e):
                group = pl.ds(pl.multiple_of(e * cap, cap), cap)
                rows = dot(pick[group, :], values[...]) * lift[group, 0:1] * gain_ref[:, col(c)]
                pk_s[s, group, col(c)] = rows.astype(BF)

        groups(local)
        pack_copy(s, c).start()
        groups(0)

    def stage_a(s, h):
        i = 2 * s + h
        if h:
            for c in range(parts):
                pack_copy(s, c).wait_recv()
        source = pk_r if h else pk_s

        @pl.loop(0, local)
        def _(j):
            group = pl.ds(pl.multiple_of(j * cap, cap), cap)
            rows = source[s, group, :]
            gate = dot(rows, gate_v[j]).astype(BF)
            upper = dot(rows, up_v[j]).astype(BF)
            for q in range(nt):
                slab = q % 2 * 2 + q // 2
                part[i, slab, group, pl.ds(0, fq)] = gate[:, q * fq:(q + 1) * fq]
                part[i, slab, group, pl.ds(fq, fq)] = upper[:, q * fq:(q + 1) * fq]

        p_copy(i).start()

    def pair_sum(i, side_row):
        return part[i, 2 * pair + side_row].astype(F32) + recv_p[i, side_row].astype(F32)

    def stage_y(s, h):
        i = 2 * s + h
        p_copy(i).wait_recv()
        pair_s[i] = pair_sum(i, 1 - row).astype(BF)
        y_copy(i).start()

    def stage_b(s, h):
        i = 2 * s + h
        y_copy(i).wait_recv()
        total = pair_sum(i, row) + pair_r[i].astype(F32)
        gate, upper = total[:, :fq], total[:, fq:]
        hid[i, my_tp] = (gate / (1.0 + jnp.exp(-gate)) * upper).astype(BF)
        for o in range(1, nt):
            h_copy(i, o).start()

    def hidden(s, h, j):
        return jnp.concatenate([hid[2 * s + h, q, pl.ds(j * cap, cap), :] for q in range(nt)], axis=1)

    def take_hidden(s, h):
        for o in range(1, nt):
            h_copy(2 * s + h, o, True).wait_recv()

    def stage_c(s):
        take_hidden(s, 0)
        for j in range(local):
            out_o[s, pl.ds(j * cap, cap), :] = dot(hidden(s, 0, j), down_v[j]).astype(BF)

    def send_back(s, c):
        if c == 0:
            take_hidden(s, 1)
        for j in range(local):
            ret_s[s, pl.ds(j * cap, cap), col(c)] = dot(hidden(s, 1, j), down_v[j, :, col(c)]).astype(BF)
        ret_copy(s, c, col).start()

    def weave(s):
        table = cols[s]
        spot = lax.broadcasted_iota(jnp.int32, (rows_all, cap), 1).astype(F32)
        for e in range(2 * local):
            here = spot == table[:, e:e + 1]
            comb[s, :, pl.ds(e * cap, cap)] = jnp.where(here, table[:, 16 + e:17 + e], 0.0).astype(BF)

    def mix(s, c, put):
        ret_copy(s, c, col).wait_recv()

        @pl.loop(0, 2)
        def _(k):
            group = pl.ds(pl.multiple_of(k * (rows_all // 2), rows_all // 2), rows_all // 2)
            near = dot(comb[s, group, pl.ds(0, count)], out_o[s, :, col(c)])
            put(group, near + dot(comb[s, group, pl.ds(count, count)], ret_r[s, :, col(c)]))

    def stage_d(s, c, more):
        if more:
            sum_wait(block(s), c, col)

        def put(group, total):
            if more:
                total = total + sum_r[block(s), group, col(c)].astype(F32)
            sum_s[s - 1, group, col(c)] = total.astype(BF)

        mix(s, c, put)
        sum_copy(s, c, col).start()

    def own_mix(c):
        def put(group, total):
            acc[group, col(c)] = total

        mix(0, c, put)

    def add_spare(c):
        sum_wait(spare, c, col)
        acc[:, col(c)] += sum_r[spare, :, col(c)].astype(F32)

    def add_last(c):
        sum_wait(z, c, col)
        acc[:, col(c)] += sum_r[z, :, col(c)].astype(F32)

    def pass_on(s, c):
        relay(s, c).wait_recv()
        relay(s, c).start()

    def pass_note(s):
        relay_note(s).wait_recv()
        relay_note(s).start()

    def arrive(s, c):
        relay(s, c).wait_recv()

    def take_note(s):
        relay_note(s).wait_recv()

    def lead(k):
        own_copy(0, k).start()

    def run(order, at_end):
        def prep(s):
            if at_end:
                take_note(s)
            prepare(s)

        def bring(s, c):
            if at_end:
                arrive(s, c)
            pack(s, c)

        calls = {
            "passn": pass_note, "pass": pass_on, "ownin": lead, "prep": prep, "pack": bring,
            "a": stage_a, "a2": stage_y, "b": stage_b, "c": stage_c, "c1": send_back, "weave": weave, "mix0": own_mix,
            "d": lambda s, c: stage_d(s, c, not at_end), "spare": add_spare, "last": add_last,
        }
        for name, *where in order:
            calls[name](*where)

    pl.semaphore_wait(barrier, jnp.where(inner, 3, 2) + nt - 1)
    x_loads[0].wait()
    own_copy(0, 0).start()

    @pl.when(inner)
    def _():
        own_copy(1, 0).start()

    for load in x_loads[1:]:
        load.wait()
    values = x_ref[...].astype(F32)
    start_sum(0, jnp.sum(values * values, axis=1, keepdims=True))
    send_sum(0)
    shape = (rows_all, rows_all)
    earlier = lax.broadcasted_iota(jnp.int32, shape, 0) < lax.broadcasted_iota(jnp.int32, shape, 1)
    tri[...] = jnp.where(earlier, 1.0, 0.0).astype(BF)
    for load in small_loads:
        load.wait()
    blank = jnp.zeros((3, rows_all), F32)
    note_s[...] = jnp.concatenate(
        [route_ref[...].astype(F32), weight_ref[...], finish_sum(0)[0:1], blank], axis=0
    )
    own_note(0).start()

    @pl.when(inner)
    def _():
        own_note(1).start()
        for c in range(1, parts // 2):
            own_copy(0, c).start()
        for c in range(1, parts):
            own_copy(1, c).start()

    @pl.when(end)
    def _():
        for c in range(1, parts):
            own_copy(0, c).start()

    prepare(0)
    for c in range(parts):
        pack(0, c)
    for load in loads:
        load.wait()

    @pl.when(end)
    def _():
        run(END_ORDER, True)

    @pl.when(inner)
    def _():
        run(INNER_ORDER, False)

    summed = acc[...]
    start_sum(1, jnp.sum(summed * summed, axis=1, keepdims=True))
    send_sum(1)

    for i in range(2 * last + 2):
        p_copy(i).wait_send()
        y_copy(i).wait_send()
        for o in range(1, nt):
            h_copy(i, o).wait_send()
    for s in range(last + 1):
        for c in range(parts):
            pack_copy(s, c).wait_send()
            ret_copy(s, c, col).wait_send()
            if s:
                sum_copy(s, c, col).wait_send()
    for c in range(parts):
        own_copy(0, c).wait_send()
    own_note(0).wait_send()

    @pl.when(inner)
    def _():
        own_note(1).wait_send()
        for c in range(parts):
            own_copy(1, c).wait_send()
        for s in range(1, last + 1):
            relay_note(s).wait_send()
            for c in range(parts):
                relay(s, c).wait_send()

    scale = jnp.sum(jnp.where(eye(), finish_sum(1)[0:1], 0.0), axis=1, keepdims=True)
    rows_k = rows_all // parts
    stores = []
    for k in range(parts):
        band = pl.ds(k * rows_k, rows_k)
        x_ref[band, :] = (acc[band, :] * scale[k * rows_k:(k + 1) * rows_k] * last_gain_ref[...]).astype(BF)
        stores.append(pltpu.make_async_copy(x_ref.at[band, :], out_hbm.at[band, :], x_sem.at[k]))
        stores[-1].start()
    for store in stores:
        store.wait()
    for k in range(2):
        for o in range(1, nt):
            sq_copy(k, o).wait_send()


def line_call(n, nt, local, cap, full, tokens, routes, weights, norm_gain, gate_weight, up_weight, down_weight, final_gain):
    rows, width = tokens.shape
    ff = gate_weight.shape[2]
    line = n // 2
    count = local * cap
    parts = 4
    any_spec = pl.BlockSpec(memory_space=pltpu.HBM)
    dma = pltpu.SemaphoreType.DMA
    return pl.pallas_call(
        functools.partial(line_kernel, n, nt, local, cap, full, parts),
        out_shape=jax.ShapeDtypeStruct((rows, width), BF),
        in_specs=[any_spec, any_spec, any_spec, any_spec, any_spec, any_spec, any_spec, any_spec],
        out_specs=any_spec,
        scratch_shapes=[
            pltpu.VMEM(gate_weight.shape, BF),
            pltpu.VMEM(up_weight.shape, BF),
            pltpu.VMEM(down_weight.shape, BF),
            pltpu.VMEM(routes.T.shape, routes.dtype),
            pltpu.VMEM(weights.T.shape, F32),
            pltpu.VMEM((1, width), F32),
            pltpu.VMEM((1, width), F32),
            pltpu.VMEM((rows, width), BF),
            pltpu.VMEM((line, rows, width), BF),
            pltpu.VMEM((line, 8, rows), F32),
            pltpu.VMEM((8, rows), F32),
            pltpu.VMEM((rows, rows), BF),
            pltpu.VMEM((line, rows, 128), F32),
            pltpu.VMEM((2 * count, rows), BF),
            pltpu.VMEM((2 * count, 128), F32),
            pltpu.VMEM((line, 2 * count, width), BF),
            pltpu.VMEM((line, count, width), BF),
            pltpu.VMEM((n, nt, count, 2 * ff // nt), BF),
            pltpu.VMEM((n, 2, count, 2 * ff // nt), BF),
            pltpu.VMEM((n, count, 2 * ff // nt), BF),
            pltpu.VMEM((n, count, 2 * ff // nt), BF),
            pltpu.VMEM((n, nt, count, ff // nt), BF),
            pltpu.VMEM((line, count, width), BF),
            pltpu.VMEM((line, count, width), BF),
            pltpu.VMEM((line, count, width), BF),
            pltpu.VMEM((line, rows, 2 * count), BF),
            pltpu.VMEM((line - 1, rows, width), BF),
            pltpu.VMEM((line + 1, rows, width), BF),
            pltpu.VMEM((rows, width), F32),
            pltpu.VMEM((2, 8, rows), F32),
            pltpu.VMEM((2, nt - 1, 8, rows), F32),
            dma((3,)),
            dma((4,)),
            dma((parts,)),
            dma((2, parts)),
            dma((line - 1, parts)),
            dma((line, parts)),
            dma((2,)),
            dma((line - 1,)),
            dma((line,)),
            dma((line, parts)),
            dma((line, parts)),
            dma((n,)),
            dma((n,)),
            dma((n,)),
            dma((n,)),
            dma((n, 3)),
            dma((n, 3)),
            dma((line, parts)),
            dma((line, parts)),
            dma((line - 1, parts)),
            dma((line + 1, parts)),
            dma((2, nt - 1)),
            dma((2, nt - 1)),
        ],
        compiler_params=pltpu.CompilerParams(
            collective_id=0, has_side_effects=True, vmem_limit_bytes=62 * 1024 * 1024
        ),
    )(tokens, routes.T, weights.T, norm_gain[None], final_gain[None], gate_weight, up_weight, down_weight)


RING_BYTES = 24 * 1024 * 1024


def body(tokens, routes, route_weights, norm_gain, gate_weight, up_weight, down_weight, final_gain):
    n, nt = lax.axis_size("ep"), lax.axis_size("tp")
    local, width, ff = gate_weight.shape
    experts = n * local
    rows = tokens.shape[0]
    full = width * nt
    cap = 4 * rows // experts
    count = local * cap
    blocks = max(n - 4, 0)
    ring = n % 2 == 0 and n >= 6 and local % 2 == 0 and blocks * rows * width * 2 <= RING_BYTES
    if n == 8 and nt == 4 and local <= 8 and width % 512 == 0 and cap % 128 == 0:
        return line_call(
            n, nt, local, cap, full, tokens, routes, route_weights, norm_gain, gate_weight, up_weight, down_weight, final_gain
        )
    meta = jnp.concatenate(
        [routes.T.astype(F32), route_weights.T, jnp.zeros((4, rows), F32)], axis=0
    )
    tables = 1 + blocks if ring else 1
    packed = count + local // 2 * cap

    any_spec = pl.BlockSpec(memory_space=pl.ANY)
    vmem = pl.BlockSpec(memory_space=pltpu.VMEM)
    dma = pltpu.SemaphoreType.DMA

    def only(ring_shape, shape, kind=BF):
        return pltpu.VMEM(ring_shape if ring else shape, kind)

    tiny = (1, 16, 128)
    return pl.pallas_call(
        functools.partial(kernel, n, nt, local, cap, ring, full),
        out_shape=jax.ShapeDtypeStruct((rows, width), BF),
        in_specs=[vmem, vmem, vmem, vmem, any_spec, any_spec, any_spec],
        out_specs=vmem,
        scratch_shapes=[
            pltpu.VMEM(gate_weight.shape, BF),
            pltpu.VMEM(up_weight.shape, BF),
            pltpu.VMEM(down_weight.shape, BF),
            pltpu.VMEM((rows, width), BF),
            pltpu.VMEM((rows, width), F32),
            pltpu.VMEM((rows, rows), BF),
            pltpu.VMEM((tables, experts, rows), F32),
            pltpu.VMEM((tables, experts, rows), F32),
            pltpu.VMEM((2, 8, rows), F32),
            pltpu.VMEM((2, nt - 1, 8, rows), F32),
            only(tiny, (n, count, width)),
            only((blocks, rows, width), (n, count, width)),
            only((2, packed, width), tiny),
            only((2, packed, width), tiny),
            only((2, local // 2 * cap, width), tiny),
            only((blocks, 8, rows), (1, 8, 128), F32),
            pltpu.VMEM((n, nt, count, 2 * ff // nt), BF),
            pltpu.VMEM((n, nt - 1, count, 2 * ff // nt), BF),
            pltpu.VMEM((n, nt, count, ff // nt), BF),
            pltpu.VMEM((n, count, width), BF),
            pltpu.VMEM((n, count, width), BF),
            dma((3,)),
            dma((blocks, 2) if ring else (n,)),
            dma((blocks, 2) if ring else (n,)),
            dma((2,)),
            dma((2,)),
            dma((2,)),
            dma((2,)),
            dma((blocks,) if ring else (1,)),
            dma((blocks,) if ring else (1,)),
            dma((n, nt - 1)),
            dma((n, nt - 1)),
            dma((n, nt - 1)),
            dma((n, nt - 1)),
            dma((n,)),
            dma((n,)),
            dma((2, nt - 1)),
            dma((2, nt - 1)),
        ],
        compiler_params=pltpu.CompilerParams(
            collective_id=0, has_side_effects=True, vmem_limit_bytes=60 * 1024 * 1024
        ),
    )(tokens, meta, norm_gain[None], final_gain[None], gate_weight, up_weight, down_weight)


def solution(mesh):
    in_specs = (
        P("ep", "tp"),
        P("ep", None),
        P("ep", None),
        P("tp"),
        P("ep", "tp", None),
        P("ep", "tp", None),
        P("ep", None, "tp"),
        P("tp"),
    )
    return jax.shard_map(body, mesh=mesh, in_specs=in_specs, out_specs=P("ep", "tp"), check_vma=False)
```
